32 devices in a mesh: sp: 8 (over z, y), tp: 4 (over x, core).
Axes of the slice: x: 2, y: 2, z: 4, core: 2. Of those that a mesh axis runs over, the one named last changes fastest.
Arguments:
- query_proj: bfloat16 [8192, 2048], P('sp', 'tp'), may hold values from -6 to 6
- key_proj: bfloat16 [8192, 2048], P('sp', 'tp'), may hold values from -6 to 6
- value_proj: bfloat16 [8192, 4096], P('sp', 'tp'), may hold values from -6 to 6
- gate_proj: bfloat16 [8192, 4096], P('sp', 'tp'), may hold values from -6 to 6
- log_decay: float32 [8192, 8], P('sp', 'tp'), may hold values from -0.75 to 0, as said below
- residual: bfloat16 [8192, 2048], P('sp'), may hold values from -4 to 4
- out_weight: bfloat16 [4096, 2048], P('tp'), may hold values from -0.09375 to 0.09375
- norm_gain: float32 [2, 2048], replicated, may hold values from 0.1 to 1.9
- norm_bias: float32 [2, 2048], replicated, may hold values from -1.5 to 1.5
- up_gate: bfloat16 [2048, 5632], P('sp', 'tp'), may hold values from -0.125 to 0.125
- up_value: bfloat16 [2048, 5632], P('sp', 'tp'), may hold values from -0.125 to 0.125
- conv_weight: float32 [2, 3, 5632], P(None, None, 'tp'), may hold values from -3 to 3
- conv_bias: float32 [2, 5632], P(None, 'tp'), may hold values from -1.5 to 1.5
- down_weight: bfloat16 [5632, 2048], P('tp', 'sp'), may hold values from -0.078125 to 0.078125
Outputs:
- layer_output: bfloat16 [8192, 2048], P(('sp', 'tp'))
The draws below stay inside these ranges and needn't reach their ends.
Inputs may be any that keep to these rules, and one draw needn't show every extreme that they name: `log_decay`: all entries are negative.
All inputs are finite; a program needn't handle non-finite values.
Results may differ from the reference program's by a relative error of at most 0.023.
Values may be sent and summed in bfloat16 or wider, within the bound.
A program may use at most 128 MiB of HBM per device.

```python
import math
import jax
import jax.numpy as jnp
from jax import lax

D = 2048
RETENTION_HEADS = 8
DK = 256
DV = 512
FF = 5632
BLOCK = 256
TOK_DEV = 1024
SEQUENCE_TOKENS = 8192
N_TP = 4


def draw_log_decay(key, part):
    random_keys = jax.random.split(jax.random.fold_in(key, 71), 7)
    fast_limit = 5
    quick_decay_heads = jax.random.randint(random_keys[0], (RETENTION_HEADS,), 0, 10) < fast_limit
    fast_span = jax.random.uniform(random_keys[1], (RETENTION_HEADS,), jnp.float32, 30.0, 50.0)
    slow_rate = -0.2 / SEQUENCE_TOKENS * jax.random.uniform(random_keys[2], (RETENTION_HEADS,), jnp.float32, 0.5, 1.0)
    decay_base_rate = jnp.where(quick_decay_heads, -math.log(10.0) / fast_span, slow_rate)
    device_count = SEQUENCE_TOKENS // TOK_DEV
    replica_multiplier = jnp.exp(jax.random.uniform(random_keys[3], (device_count, RETENTION_HEADS), jnp.float32, math.log(0.5), math.log(2.0)))
    replica_multiplier = jnp.repeat(replica_multiplier, TOK_DEV, axis=0)
    jitter_amount = jax.random.uniform(random_keys[4], (SEQUENCE_TOKENS, RETENTION_HEADS), jnp.float32, 0.5, 1.5)
    spike_positions = jax.random.randint(random_keys[5], (2, RETENTION_HEADS), 0, SEQUENCE_TOKENS)
    spike_lengths = jax.random.uniform(random_keys[6], (2, RETENTION_HEADS), jnp.float32, math.log(0.5), math.log(0.8))
    position_slots = jnp.arange(SEQUENCE_TOKENS)[:, None]
    spike_events = jnp.where(position_slots == spike_positions[0][None, :], spike_lengths[0][None, :], 0.0)
    spike_events = spike_events + jnp.where(position_slots == spike_positions[1][None, :], spike_lengths[1][None, :], 0.0)
    spike_events = jnp.where(quick_decay_heads[None, :], 0.0, spike_events)
    return (decay_base_rate[None, :] * replica_multiplier * jitter_amount + spike_events).astype(jnp.float32)


def shard_levels(rng, extent, cuts, least, largest):
    def one(position, parts):
        steps = jax.random.uniform(jax.random.fold_in(jax.random.fold_in(rng, 6), position), (parts,), jnp.float32, least / len(cuts), largest / len(cuts))
        return jnp.repeat(jnp.exp(steps), extent[position] // parts).reshape((-1,) + (1,) * (len(extent) - position - 1))

    loudness = one(*cuts[0])
    for cut in cuts[1:]:
        loudness = loudness * one(*cut)
    return loudness


def normal_values(own_key, dims, deviation, limit, cuts=(), held_as=jnp.bfloat16):
    values = jax.random.normal(own_key, dims, jnp.float32) * deviation
    if len(cuts) > 0:
        values = shard_levels(own_key, dims, cuts, -0.22, 0.18) * values
    return jnp.clip(values, min=-limit, max=limit).astype(held_as)


def setup_inputs(seed: int = 0) -> dict:
    splits = jax.random.split(jax.random.key(seed), 15)
    query_proj = normal_values(splits[0], (SEQUENCE_TOKENS, RETENTION_HEADS * DK), 1.0, 6.0, ((0, 8), (1, 4)))
    key_proj = normal_values(splits[1], (SEQUENCE_TOKENS, RETENTION_HEADS * DK), 1.0, 6.0, ((0, 8), (1, 4)))
    value_proj = normal_values(splits[2], (SEQUENCE_TOKENS, RETENTION_HEADS * DV), 1.0, 6.0, ((0, 8), (1, 4)))
    gate_proj = normal_values(splits[3], (SEQUENCE_TOKENS, RETENTION_HEADS * DV), 1.0, 6.0, ((0, 8), (1, 4)))
    log_decay = draw_log_decay(jax.random.fold_in(splits[14], 71), 0)
    residual = normal_values(splits[5], (SEQUENCE_TOKENS, D), 0.5, 4.0, ((0, 8),))
    out_weight = normal_values(splits[6], (RETENTION_HEADS * DV, D), (RETENTION_HEADS * DV) ** -0.5, 0.09375, ((0, 4),))
    norm_gain = jnp.clip(1.0 + 0.18 * jax.random.normal(splits[7], (2, D), jnp.float32), 0.1, 1.9)
    norm_bias = normal_values(splits[8], (2, D), 0.3, 1.5, (), jnp.float32)
    up_gate = normal_values(splits[9], (D, FF), D ** -0.5, 0.125, ((0, 8), (1, 4)))
    up_value = normal_values(splits[10], (D, FF), D ** -0.5, 0.125, ((0, 8), (1, 4)))
    conv_weight = normal_values(splits[11], (2, 3, FF), 0.577, 3.0, ((2, 4),), jnp.float32)
    conv_bias = normal_values(splits[12], (2, FF), 0.3, 1.5, ((1, 4),), jnp.float32)
    down_weight = normal_values(splits[13], (FF, D), FF ** -0.5, 0.078125, ((0, 4), (1, 8)))
    return dict(query_proj=query_proj, key_proj=key_proj, value_proj=value_proj, gate_proj=gate_proj, log_decay=log_decay, residual=residual, out_weight=out_weight, norm_gain=norm_gain, norm_bias=norm_bias, up_gate=up_gate, up_value=up_value, conv_weight=conv_weight, conv_bias=conv_bias, down_weight=down_weight)


alpha_scale = 8.0 ** 0.25
rope_base = 10000.0
tiny_stabilizer = 1e-05

def rotate(vectors, positions):
    head_width = vectors.shape[-1]
    half_width = head_width // 2
    inverse_freq = rope_base ** (-2.0 * jnp.arange(half_width, dtype=jnp.float32) / head_width)
    angles = positions[:, None] * inverse_freq[None, :]
    cosine = jnp.cos(angles)[:, None, :]
    sine_part = jnp.sin(angles)[:, None, :]
    front = vectors[..., :half_width]
    second = vectors[..., half_width:]
    return jnp.concatenate([front * cosine - second * sine_part, front * sine_part + second * cosine], axis=-1)

def layer_norm(values, gain, shift):
    average = values.mean(-1, keepdims=True)
    spread = jnp.square(values - average).mean(-1, keepdims=True)
    return (values - average) * lax.rsqrt(spread + tiny_stabilizer) * gain + shift

def rounded(values):
    return lax.optimization_barrier(values.astype(jnp.bfloat16)).astype(jnp.float32)

def block_parts(query_tile, lookup_piece, payload_piece, log_blk):
    cum_log = jnp.cumsum(log_blk, axis=0)
    cum_heads = cum_log.T
    log_gap = cum_heads[:, :, None] - cum_heads[:, None, :]
    offsets = jnp.arange(log_blk.shape[0])
    causal = (offsets[:, None] >= offsets[None, :])[None]
    weight = jnp.where(causal, jnp.exp(jnp.where(causal, log_gap, 0.0)), 0.0)
    score_matrix = jnp.einsum('jka,ska->kjs', query_tile.astype(jnp.float32), lookup_piece.astype(jnp.float32))
    segment_scaling = (score_matrix * weight).astype(jnp.bfloat16)
    within = jnp.einsum('htm,mhe->the', segment_scaling.astype(jnp.float32), payload_piece.astype(jnp.float32))
    block_total = cum_log[-1]
    to_end = jnp.exp(block_total[None, :] - cum_log)
    faded_lookup_vector = rounded(lookup_piece.astype(jnp.float32) * to_end[:, :, None])
    summand_term = jnp.einsum('ajo,ajd->jod', faded_lookup_vector, payload_piece.astype(jnp.float32), precision=lax.Precision.HIGHEST)
    scaled_query = rounded(query_tile.astype(jnp.float32) * jnp.exp(cum_log)[:, :, None])
    return (within, scaled_query, summand_term, jnp.exp(block_total))

def grouped_product(left, right, group_count):
    group_width = left.shape[1] // group_count
    left_groups = left.reshape(left.shape[0], group_count, group_width).transpose(1, 0, 2)
    right_groups = right.reshape(group_count, group_width, right.shape[1])

    def add_group(total, pieces):
        term = jnp.dot(pieces[0], pieces[1], preferred_element_type=jnp.float32).astype(jnp.bfloat16)
        return (total + term.astype(jnp.float32), None)
    blank_sum = jnp.zeros((left.shape[0], right.shape[1]), jnp.float32)
    total, _ = lax.scan(add_group, blank_sum, (left_groups, right_groups))
    return total

def causal_conv(rows, taps, shift):
    padded = jnp.pad(rows.astype(jnp.float32), ((2, 0), (0, 0)))
    length = rows.shape[0]
    result = shift[None, :] + padded[0:length] * taps[0]
    result = result + padded[1:length + 1] * taps[1]
    return result + padded[2:length + 2] * taps[2]

def reference(query_proj, key_proj, value_proj, gate_proj, log_decay, residual, out_weight, norm_gain, norm_bias, up_gate, up_value, conv_weight, conv_bias, down_weight):
    length = query_proj.shape[0]
    positions = jnp.arange(length).astype(jnp.float32)
    query_rot = rotate(query_proj.astype(jnp.float32).reshape(length, RETENTION_HEADS, DK), positions).astype(jnp.bfloat16)
    key_rot = (rotate(key_proj.astype(jnp.float32).reshape(length, RETENTION_HEADS, DK), positions) * DK ** (-0.5)).astype(jnp.bfloat16)
    block_count = length // BLOCK
    asking_segments = query_rot.reshape(block_count, BLOCK, RETENTION_HEADS, DK)
    key_blocks = key_rot.reshape(block_count, BLOCK, RETENTION_HEADS, DK)
    value_blocks = value_proj.reshape(block_count, BLOCK, RETENTION_HEADS, DV)
    log_blocks = log_decay.reshape(block_count, BLOCK, RETENTION_HEADS)

    def advance(carry_state, pieces):
        within, scaled_query, summand_term, block_decay = block_parts(*pieces)
        carried = jnp.einsum('thd,hde->the', scaled_query, rounded(carry_state), precision=lax.Precision.HIGHEST)
        return (block_decay[:, None, None] * carry_state + summand_term, within + carried)
    start_state = jnp.zeros((RETENTION_HEADS, DK, DV), jnp.float32)
    _, mixed_heads = lax.scan(advance, start_state, (asking_segments, key_blocks, value_blocks, log_blocks))
    mixed_heads = mixed_heads.reshape(length, RETENTION_HEADS, DV)
    average = mixed_heads.mean(-1, keepdims=True)
    spread = jnp.square(mixed_heads - average).mean(-1, keepdims=True)
    standardized_rows = (mixed_heads - average) * lax.rsqrt(spread + tiny_stabilizer)
    gate_heads = gate_proj.astype(jnp.float32).reshape(length, RETENTION_HEADS, DV)
    gated_rows = (jax.nn.silu(gate_heads) * standardized_rows).astype(jnp.bfloat16).reshape(length, RETENTION_HEADS * DV)
    attended = grouped_product(gated_rows, out_weight, N_TP)
    normed_rows = layer_norm(alpha_scale * residual.astype(jnp.float32) + attended, norm_gain[0], norm_bias[0]).astype(jnp.bfloat16)
    gate_up = jnp.dot(normed_rows, up_gate, preferred_element_type=jnp.float32).astype(jnp.bfloat16)
    value_up = jnp.dot(normed_rows, up_value, preferred_element_type=jnp.float32).astype(jnp.bfloat16)
    gate_conv = causal_conv(gate_up, conv_weight[0], conv_bias[0])
    value_conv = causal_conv(value_up, conv_weight[1], conv_bias[1])
    activated = (jax.nn.gelu(gate_conv) * value_conv).astype(jnp.bfloat16)
    ffn_out = grouped_product(activated, down_weight, N_TP)
    return layer_norm(alpha_scale * normed_rows.astype(jnp.float32) + ffn_out, norm_gain[1], norm_bias[1]).astype(jnp.bfloat16)
```

```python
import numpy as np
import jax
import jax.numpy as jnp
from jax import lax
from jax.experimental import pallas as pl
from jax.experimental.pallas import tpu as pltpu
from jax.sharding import PartitionSpec as P

BLOCK = 256
HALO = 16
ROW_CHUNKS = 4

alpha_scale = 8.0**0.25
rope_base = 10000.0
tiny_stabilizer = 1e-05
MESH = pl.DeviceIdType.MESH
F32, BF16 = jnp.float32, jnp.bfloat16


def dot(a, b):
    return jnp.dot(a, b, preferred_element_type=F32)


def dot_t(a, b, dims, precision=None):
    return lax.dot_general(a, b, (dims, ((), ())), precision=precision, preferred_element_type=F32)


def layout(sp, tp):
    cores = 2 if tp % 2 == 0 else 1
    lines = tp // cores
    ny = lines if sp % lines == 0 else 1
    return cores, lines, ny, sp // ny


def rotary_tables(head_width, blocks):
    half = head_width // 2
    freq = rope_base ** (-2.0 * np.arange(half, dtype=np.float64) / head_width)
    inner = np.arange(BLOCK, dtype=np.float64)[:, None] * freq
    outer = (np.arange(blocks, dtype=np.float64) * BLOCK)[:, None] * freq
    tables = (np.cos(inner), np.sin(inner), np.cos(outer), np.sin(outer))
    return [jnp.asarray(t.astype(np.float32)) for t in tables]


class Sends:
    def __init__(self):
        self.left = []

    def start(self, copy, cond=None):
        self.left.append((copy, cond))
        if cond is None:
            copy.start()
        else:
            pl.when(cond)(copy.start)

    def drain(self):
        for copy, cond in self.left:
            if cond is None:
                copy.wait_send()
            else:
                pl.when(cond)(copy.wait_send)
        self.left = []


def make_kernel(n_sp, n_tp, tok_rows, heads, key_width, value_width, width, depth, hidden):
    cores, lines, ny, nz = layout(n_sp, n_tp)
    nb = tok_rows // BLOCK
    own = tok_rows // n_tp
    piece = width // n_sp
    slice_w = value_width // ny
    half_k = key_width // 2
    dh, hh = depth // 2, hidden // 2
    chunk = own // ROW_CHUNKS
    hcols = 128 if hidden % 128 == 0 else hidden

    def kernel(
        cos_in, sin_in, cos_out, sin_out, log_ref, gain, bias, taps, shift,
        q_hbm, k_hbm, v_hbm, g_hbm, res_hbm, ow_hbm, upg, upv, down,
        out,
        wg, wd, qb, kb, vb, gb, ow, res, cum_col, st, lb, within,
        xs, xr, dec, chain_s, chain_r, cb, cs, part, r1, s2, r2, acc, rows, ups, act,
        load_sem, bulk_r, bulk_z, bulk_y, st_s, st_r, dec_s, dec_r, ch_s, ch_r, cb_s, cb_r,
        rs1_s, rs1_r, rs2_s, rs2_r, ag_s, ag_r, agf_s, halo_s, halo_r,
    ):
        sp, tp = lax.axis_index("sp"), lax.axis_index("tp")
        z, y = sp // ny, sp % ny
        x, c = tp // cores, tp % cores
        me_sp = sp

        def remote(src, dst, ssem, rsem, to_sp, to_tp):
            return pltpu.make_async_remote_copy(
                src_ref=src, dst_ref=dst, send_sem=ssem, recv_sem=rsem,
                device_id=(to_sp, to_tp), device_id_type=MESH,
            )

        def arrived(dst, ssem, rsem, cond=None):
            copy = remote(dst, dst, ssem, rsem, sp, tp)
            if cond is None:
                copy.wait_recv()
            else:
                pl.when(cond)(copy.wait_recv)

        own_rows = pl.ds(pl.multiple_of(tp * own, own), own)
        pairs = [
            (k_hbm, kb), (v_hbm, vb), (q_hbm, qb), (g_hbm, gb), (ow_hbm, ow),
            (res_hbm.at[own_rows], res), (upg, wg.at[me_sp, 0]), (upv, wg.at[me_sp, 1]),
            (down, wd.at[me_sp]),
        ]
        loads = [pltpu.make_async_copy(a, b, load_sem.at[i]) for i, (a, b) in enumerate(pairs)]
        for load in loads:
            load.start()

        barrier = pltpu.get_barrier_semaphore()

        def greet(to_sp, to_tp, cond=None):
            def go():
                pl.semaphore_signal(barrier, inc=1, device_id=(to_sp, to_tp), device_id_type=MESH)

            if cond is None:
                go()
            else:
                pl.when(cond)(go)

        other_y = [z * ny + (y + d) % ny for d in range(1, ny)]
        other_c = [x * cores + (c + d) % cores for d in range(1, cores)]
        other_x = [(x + d) % lines * cores + c for d in range(1, lines)]
        peers = [(sp + ny, tp, z < nz - 1), (sp - ny, tp, z > 0)]
        peers += [(o, tp, None) for o in other_y]
        peers += [(sp, o, None) for o in other_c + other_x]
        for t in range(n_tp):
            peers.append((sp + 1, t, jnp.logical_and(tp == n_tp - 1, sp < n_sp - 1)))
        for to_sp, to_tp, cond in peers:
            greet(to_sp, to_tp, cond)
        greet(sp - 1, n_tp - 1, sp > 0)
        count = (sp > 0).astype(jnp.int32)
        for _, _, cond in peers:
            count = count + (1 if cond is None else cond.astype(jnp.int32))
        pl.semaphore_wait(barrier, count)

        bulk = Sends()

        def slot(p, src):
            m, h = p // 2, p % 2
            if m < 2:
                return wg.at[src, m, pl.ds(h * dh, dh)]
            return wd.at[src, pl.ds(h * hh, hh)]

        def mine(p):
            m, h = p // 2, p % 2
            if m == 2:
                return down.at[pl.ds(h * hh, hh)]
            return (upg, upv)[m].at[pl.ds(h * dh, dh)]

        def own_z(p, up):
            cond, to = (z < nz - 1, sp + ny) if up else (z > 0, sp - ny)
            bulk.start(
                remote(mine(p), slot(p, sp), bulk_z.at[p, 0 if up else 1], bulk_r.at[p, sp], to, tp),
                cond,
            )

        def own_y(p):
            for d, to in enumerate(other_y):
                bulk.start(
                    remote(mine(p), slot(p, sp), bulk_y.at[p, 0, d], bulk_r.at[p, sp], to, tp)
                )

        def source(up, d):
            return (sp - d * ny, z >= d) if up else (sp + d * ny, z < nz - d)

        def take(p, up, d):
            src, cond = source(up, d)
            src = jnp.clip(src, 0, n_sp - 1)
            arrived(slot(p, src), bulk_z.at[p, 0], bulk_r.at[p, src], cond)

        def on_z(p, up, d):
            src, cond = source(up, d)
            src = jnp.clip(src, 0, n_sp - 1)
            to, more = (sp + ny, z < nz - 1) if up else (sp - ny, z > 0)
            sem = bulk_z.at[p, 2 * d + (0 if up else 1)]
            bulk.start(
                remote(slot(p, src), slot(p, src), sem, bulk_r.at[p, src], to, tp),
                jnp.logical_and(cond, more),
            )

        def on_y(p, up, d):
            src, cond = source(up, d)
            src = jnp.clip(src, 0, n_sp - 1)
            for e, to in enumerate(other_y):
                sem = bulk_y.at[p, 2 * d + (0 if up else 1), e]
                bulk.start(
                    remote(slot(p, src), slot(p, src), sem, bulk_r.at[p, src], to, tp), cond
                )

        def relay(m, up, d):
            if d >= nz:
                return
            for p in (2 * m, 2 * m + 1):
                take(p, up, d)
                if d < nz - 1:
                    on_z(p, up, d)
                on_y(p, up, d)

        def side_arrivals(m):
            for src in range(n_sp):
                for p in (2 * m, 2 * m + 1):
                    arrived(slot(p, src), bulk_z.at[p, 0], bulk_r.at[p, src], src % ny != y)

        for p in (0, 1):
            own_z(p, True)
        for p in (0, 1, 2, 3):
            own_z(p, False)
        own_y(0)

        ii = lax.broadcasted_iota(jnp.int32, (BLOCK, BLOCK), 0)
        jj = lax.broadcasted_iota(jnp.int32, (BLOCK, BLOCK), 1)
        lower = (ii >= jj).astype(F32)
        logs = log_ref[...]
        cum_col[...] = dot_t(lower, logs, ((1,), (1,)), lax.Precision.HIGHEST)

        def column(idx):
            lane = lax.broadcasted_iota(jnp.int32, cum_col.shape, 1)
            return jnp.sum(jnp.where(lane == idx, cum_col[...], 0.0), axis=1, keepdims=True)

        def angles(b):
            row = pl.ds(sp * nb + b, 1)
            co, so = cos_out[row, :], sin_out[row, :]
            ci, si = cos_in[...], sin_in[...]
            return ci * co - si * so, si * co + ci * so

        def rotated(value, cosine, sine):
            front, second = value[:, :half_k], value[:, half_k:]
            return jnp.concatenate(
                [front * cosine - second * sine, front * sine + second * cosine], axis=1
            )

        def block_rows(b):
            return pl.ds(pl.multiple_of(b * BLOCK, BLOCK), BLOCK)

        loads[0].wait()
        loads[1].wait()
        st[...] = jnp.zeros_like(st)

        def local_states(b, _):
            r = block_rows(b)
            cosine, sine = angles(b)
            for h in range(heads):
                cc = column(h * nb + b)
                total = cc[BLOCK - 1 : BLOCK, :]
                kc = pl.ds(h * key_width, key_width)
                key = rotated(kb[r, kc].astype(F32), cosine, sine) * key_width ** (-0.5)
                key = key.astype(BF16)
                kb[r, kc] = key
                faded = (key.astype(F32) * jnp.exp(total - cc)).astype(BF16)
                term = dot_t(faded, vb[r, pl.ds(h * value_width, value_width)], ((0,), (0,)))
                before = st[h]
                lb[b * heads + h] = before.astype(BF16)
                st[h] = jnp.exp(total) * before + term
            return 0

        lax.fori_loop(0, nb, local_states, 0)

        def head_log(h):
            total = jnp.zeros((1, 1), F32)
            for b in range(nb):
                total = total + jnp.sum(logs[h * nb + b : h * nb + b + 1, :], axis=1, keepdims=True)
            return total

        hrow = lax.broadcasted_iota(jnp.int32, (8, 128), 0)
        tile = jnp.zeros((8, 128), F32)
        for h in range(heads):
            tile = jnp.where(hrow == h, head_log(h), tile)
        dec[pl.ds(y, 1)] = tile[None]
        states = Sends()
        for d, to in enumerate(other_y):
            far = (y + d + 1) % ny
            states.start(
                remote(dec.at[y], dec.at[y], dec_s.at[d], dec_r.at[y], to, tp)
            )
            for h in range(heads):
                for f in range(ny):

                    @pl.when(far == f)
                    def _():
                        xs[d, h] = st[h, :, f * slice_w : (f + 1) * slice_w].astype(BF16)

                states.start(
                    remote(xs.at[d, h], xr.at[y, h], st_s.at[d, h], st_r.at[y, h], to, tp)
                )
        for p in (1, 2, 3):
            own_y(p)

        loads[2].wait()

        def within_block(b, _):
            r = block_rows(b)
            cosine, sine = angles(b)
            for h in range(heads):
                cc = column(h * nb + b)
                kc = pl.ds(h * key_width, key_width)
                query = rotated(qb[r, kc].astype(F32), cosine, sine).astype(BF16)
                scores = dot_t(query, kb[r, kc], ((1,), (1,)))
                crow = jnp.sum(jnp.where(ii == jj, cc, 0.0), axis=0, keepdims=True)
                gap = jnp.where(ii >= jj, cc - crow, 0.0)
                weight = jnp.where(ii >= jj, jnp.exp(gap), 0.0)
                vc = pl.ds(h * value_width, value_width)
                within[r, vc] = dot((scores * weight).astype(BF16), vb[r, vc])
                qb[r, kc] = (query.astype(F32) * jnp.exp(cc)).astype(BF16)
            return 0

        lax.fori_loop(0, nb, within_block, 0)

        for p in (0, 1):
            take(p, False, 1)
            if nz > 2:
                on_z(p, False, 1)

        for f in range(ny):

            @pl.when(y == f)
            def _():
                for h in range(heads):
                    xr[f, h] = st[h, :, f * slice_w : (f + 1) * slice_w].astype(BF16)

        for d in range(1, ny):
            src = (y + d) % ny
            arrived(dec.at[src], dec_s.at[0], dec_r.at[src])
            for h in range(heads):
                arrived(xr.at[src, h], st_s.at[0, 0], st_r.at[src, h])
        for h in range(heads):

            @pl.when(z == 0)
            def _():
                chain_r[h] = jnp.zeros((key_width, slice_w), BF16)

            arrived(chain_r.at[h], ch_s.at[h], ch_r.at[h], z > 0)
            incoming = chain_r[h].astype(F32)
            before = incoming
            for f in range(ny):
                cb_mine = before.astype(BF16)

                @pl.when(y == f)
                def _():
                    cb[y, h] = cb_mine

                @pl.when(y != f)
                def _():
                    cs[f, h] = cb_mine

                decay = jnp.exp(dec[f, h : h + 1, 0:1])
                before = decay * before + xr[f, h].astype(F32)
            chain_s[h] = before.astype(BF16)
            states.start(
                remote(chain_s.at[h], chain_r.at[h], ch_s.at[h], ch_r.at[h], sp + ny, tp),
                z < nz - 1,
            )
            for d, to in enumerate(other_y):
                far = (y + d + 1) % ny
                states.start(
                    remote(cs.at[far, h], cb.at[y, h], cb_s.at[d, h], cb_r.at[y, h], to, tp)
                )

        for p in (2, 3):
            own_z(p, True)
        for p in (0, 1):
            on_y(p, False, 1)
            take(p, True, 1)
            if nz > 2:
                on_z(p, True, 1)
            on_y(p, True, 1)

        loads[3].wait()
        for h in range(heads):
            for d in range(1, ny):
                src = (y + d) % ny
                arrived(cb.at[src, h], cb_s.at[0, 0], cb_r.at[src, h])

            def finish(b, decay):
                r = block_rows(b)
                vc = pl.ds(h * value_width, value_width)
                state = jnp.concatenate([cb[f, h].astype(F32) for f in range(ny)], axis=1)
                state = (decay * state + lb[b * heads + h].astype(F32)).astype(BF16)
                mixed = within[r, vc] + dot(qb[r, pl.ds(h * key_width, key_width)], state)
                average = jnp.mean(mixed, axis=1, keepdims=True)
                mixed = mixed - average
                spread = jnp.mean(mixed * mixed, axis=1, keepdims=True)
                gate = gb[r, vc].astype(F32)
                gated = gate * jax.nn.sigmoid(gate) * (mixed * lax.rsqrt(spread + tiny_stabilizer))
                gb[r, vc] = gated.astype(BF16)
                return decay * jnp.exp(column(h * nb + b)[BLOCK - 1 : BLOCK, :])

            lax.fori_loop(0, nb, finish, jnp.ones((1, 1), F32))
        states.drain()

        def owner_rows(xx, cc):
            return pl.ds(pl.multiple_of((xx * cores + cc) * own, own), own)

        def piece_cols(s):
            return pl.ds(pl.multiple_of(s * piece, piece), piece)

        def d2d_copies(s):
            return [
                remote(
                    part.at[s, owner_rows(xx, (c + d) % cores)], r1.at[s, d - 1, xx],
                    rs1_s.at[s, d - 1, xx], rs1_r.at[s, d - 1, xx],
                    sp, x * cores + (c + d) % cores,
                )
                for d in range(1, cores)
                for xx in range(lines)
            ]

        def x_copies(s):
            return [
                remote(
                    s2.at[s, d - 1], r2.at[s, d - 1], rs2_s.at[s, d - 1], rs2_r.at[s, d - 1],
                    sp, (x + d) % lines * cores + c,
                )
                for d in range(1, lines)
            ]

        row_tile = min(tok_rows, 512)

        def product(s, lhs, rhs):
            def one(i, _):
                r = pl.ds(pl.multiple_of(i * row_tile, row_tile), row_tile)
                part[s, r, :] = dot(lhs[r, :], rhs()).astype(BF16)
                return 0

            lax.fori_loop(0, tok_rows // row_tile, one, 0)
            for copy in d2d_copies(s):
                copy.start()

        def combine(s):
            for copy in d2d_copies(s):
                copy.wait_recv()
            for d in range(lines):
                xx = (x + d) % lines
                total = part[s, owner_rows(xx, c), :].astype(F32)
                for e in range(cores - 1):
                    total = total + r1[s, e, xx].astype(F32)
                if d == 0:
                    acc[:, piece_cols(s)] = total
                else:
                    s2[s, d - 1] = total.astype(BF16)
            for copy in x_copies(s):
                copy.start()

        def collect(s):
            for copy in x_copies(s):
                copy.wait_recv()
            total = acc[:, piece_cols(s)]
            for d in range(lines - 1):
                total = total + r2[s, d].astype(F32)
            acc[:, piece_cols(s)] = total

        def release(s, _):
            for copy in d2d_copies(s) + x_copies(s):
                copy.wait_send()
            return 0

        def out_step(s, _):
            product(s, gb, lambda: ow[:, piece_cols(s)])
            pl.when(s > 0)(lambda: combine(s - 1))
            return 0

        loads[4].wait()
        mid = n_sp // 2
        lax.fori_loop(0, mid, out_step, 0)
        relay(1, False, 1)
        lax.fori_loop(mid, n_sp, out_step, 0)
        combine(n_sp - 1)
        relay(0, False, 2)
        relay(1, True, 1)

        def collect_step(s, _):
            collect(s)
            return 0

        lax.fori_loop(0, n_sp, collect_step, 0)
        relay(0, True, 2)

        loads[5].wait()

        def layer_norm(values, which):
            average = jnp.mean(values, axis=1, keepdims=True)
            values = values - average
            spread = jnp.mean(values * values, axis=1, keepdims=True)
            values = values * lax.rsqrt(spread + tiny_stabilizer)
            return values * gain[which : which + 1, :] + bias[which : which + 1, :]

        ln_rows = 16
        gathered = Sends()

        def chunk_of(owner, j):
            return rows.at[pl.ds(pl.multiple_of(HALO + owner * own + j * chunk, 16), chunk)]

        pl.when(sp == 0)(lambda: rows.__setitem__((pl.ds(0, HALO), slice(None)), jnp.zeros((HALO, width), BF16)))
        for j in range(ROW_CHUNKS):

            def norm_rows(i, _):
                at = pl.multiple_of(j * chunk + i * ln_rows, ln_rows)
                r = pl.ds(at, ln_rows)
                value = layer_norm(alpha_scale * res[r, :].astype(F32) + acc[r, :], 0).astype(BF16)
                res[r, :] = value
                rows[pl.ds(pl.multiple_of(HALO + tp * own + at, 16), ln_rows), :] = value
                return 0

            lax.fori_loop(0, chunk // ln_rows, norm_rows, 0)
            for d, to in enumerate(other_c + other_x):
                gathered.start(
                    remote(chunk_of(tp, j), chunk_of(tp, j), ag_s.at[j, d], ag_r.at[j, tp], sp, to)
                )
        last = pl.ds(tok_rows, HALO)
        for t in range(n_tp):
            gathered.start(
                remote(rows.at[last], rows.at[pl.ds(0, HALO)], halo_s.at[t], halo_r, sp + 1, t),
                jnp.logical_and(tp == n_tp - 1, sp < n_sp - 1),
            )
        relay(0, False, 3)
        for j in range(ROW_CHUNKS):
            for d in range(1, lines):
                owner = (x + d) % lines * cores + c
                arrived(chunk_of(owner, j), ag_s.at[j, 0], ag_r.at[j, owner])
                for e, to in enumerate(other_c):
                    gathered.start(
                        remote(
                            chunk_of(owner, j), chunk_of(owner, j),
                            agf_s.at[j, d - 1, e], ag_r.at[j, owner], sp, to,
                        )
                    )
            if j == 1:
                relay(1, False, 2)
                relay(0, True, 3)
        for d in range(1, cores):
            for e in range(lines):
                owner = (x + e) % lines * cores + (c + d) % cores
                for j in range(ROW_CHUNKS):
                    arrived(chunk_of(owner, j), ag_s.at[j, 0], ag_r.at[j, owner])
        relay(1, True, 2)
        relay(1, False, 3)
        for p in (4, 5):
            own_z(p, True)
            own_z(p, False)
        lax.fori_loop(0, n_sp, release, 0)

        def up_tile(m, start, count):
            r = pl.ds(start, count)
            total = None
            for s in range(n_sp):
                term = dot(rows[r, s * depth : (s + 1) * depth], wg[s, m])
                total = term if total is None else total + term
            ups[m, r, :] = total.astype(BF16)

        def up_rows(m):
            def one(i, _):
                up_tile(m, pl.multiple_of(HALO + i * BLOCK, 16), BLOCK)
                return 0

            lax.fori_loop(0, tok_rows // BLOCK, one, 0)
            up_tile(m, 0, HALO)

        loads[6].wait()
        side_arrivals(0)
        arrived(rows.at[pl.ds(0, HALO)], halo_s.at[0], halo_r, sp > 0)
        up_rows(0)
        relay(1, True, 3)
        for p in (4, 5):
            own_y(p)
        loads[7].wait()
        side_arrivals(1)
        up_rows(1)

        def activate(i, col):
            at = pl.multiple_of(i * BLOCK, BLOCK)
            convs = []
            for m in range(2):
                tile = ups[m, pl.ds(at, BLOCK + HALO), col].astype(F32)
                value = shift[m : m + 1, col]
                for j in range(3):
                    value = value + taps[m, j : j + 1, col] * tile[HALO - 2 + j : HALO - 2 + j + BLOCK, :]
                convs.append(value)
            act[pl.ds(at, BLOCK), col] = (jax.nn.gelu(convs[0]) * convs[1]).astype(BF16)

        def activate_step(i, _):
            for t in range(hidden // hcols):
                activate(i, pl.ds(t * hcols, hcols))
            return 0

        lax.fori_loop(0, tok_rows // BLOCK, activate_step, 0)

        order = [
            [zz] + sorted((o for o in range(nz) if o != zz), key=lambda o: (abs(o - zz), abs(2 * o - nz + 1)))
            for zz in range(nz)
        ]

        def nearest(k):
            got = jnp.int32(order[0][k])
            for zz in range(1, nz):
                got = jnp.where(z == zz, order[zz][k], got)
            return got

        steps = [(k, 0) for k in range(nz)] + [(k, d) for k in range(nz) for d in range(1, ny)]
        loads[8].wait()
        previous = None
        done = []
        for k, d in steps:
            src_z = nearest(k)
            src = src_z * ny + (y + d) % ny
            if d > 0 or k > 0:
                for p in (4, 5):
                    arrived(slot(p, src), bulk_z.at[p, 0], bulk_r.at[p, src])
            if d == 0 and k > 0:
                to_z = jnp.where(src_z < z, z + 1, z - 1)
                more = jnp.logical_and(to_z >= 0, to_z < nz)
                for p in (4, 5):
                    bulk.start(
                        remote(slot(p, src), slot(p, src), bulk_z.at[p, 1 + k], bulk_r.at[p, src], to_z * ny + y, tp),
                        more,
                    )
                    for e, to in enumerate(other_y):
                        bulk.start(
                            remote(slot(p, src), slot(p, src), bulk_y.at[p, k, e], bulk_r.at[p, src], to, tp)
                        )
            product(src, act, lambda: wd[src])
            if previous is not None:
                combine(previous)
            previous = src
            done.append(src)
        combine(previous)
        for src in done:
            collect(src)

        def final_rows(i, _):
            r = pl.ds(pl.multiple_of(i * ln_rows, ln_rows), ln_rows)
            out[r, :] = layer_norm(alpha_scale * res[r, :].astype(F32) + acc[r, :], 1).astype(BF16)
            return 0

        lax.fori_loop(0, own // ln_rows, final_rows, 0)
        lax.fori_loop(0, n_sp, release, 0)
        gathered.drain()
        bulk.drain()

    vmem, dma = pltpu.VMEM, pltpu.SemaphoreType.DMA
    oc, ol, oy = max(cores - 1, 1), max(lines - 1, 1), max(ny - 1, 1)
    scratch = [
        vmem((n_sp, 2, depth, hidden), BF16),
        vmem((n_sp, hidden, piece), BF16),
        vmem((tok_rows, heads * key_width), BF16),
        vmem((tok_rows, heads * key_width), BF16),
        vmem((tok_rows, heads * value_width), BF16),
        vmem((tok_rows, heads * value_width), BF16),
        vmem((heads * value_width, width), BF16),
        vmem((own, width), BF16),
        vmem((BLOCK, heads * nb), F32),
        vmem((heads, key_width, value_width), F32),
        vmem((nb * heads, key_width, value_width), BF16),
        vmem((tok_rows, heads * value_width), F32),
        vmem((oy, heads, key_width, slice_w), BF16),
        vmem((ny, heads, key_width, slice_w), BF16),
        vmem((ny, 8, 128), F32),
        vmem((heads, key_width, slice_w), BF16),
        vmem((heads, key_width, slice_w), BF16),
        vmem((ny, heads, key_width, slice_w), BF16),
        vmem((ny, heads, key_width, slice_w), BF16),
        vmem((n_sp, tok_rows, piece), BF16),
        vmem((n_sp, oc, lines, own, piece), BF16),
        vmem((n_sp, ol, own, piece), BF16),
        vmem((n_sp, ol, own, piece), BF16),
        vmem((own, width), F32),
        vmem((HALO + tok_rows, width), BF16),
        vmem((2, HALO + tok_rows, hidden), BF16),
        vmem((tok_rows, hidden), BF16),
        dma((9,)),
        dma((6, n_sp)),
        dma((6, 2 * nz)),
        dma((6, 2 * nz, oy)),
        dma((oy, heads)),
        dma((ny, heads)),
        dma((oy,)),
        dma((ny,)),
        dma((heads,)),
        dma((heads,)),
        dma((oy, heads)),
        dma((ny, heads)),
        dma((n_sp, oc, lines)),
        dma((n_sp, oc, lines)),
        dma((n_sp, ol)),
        dma((n_sp, ol)),
        dma((ROW_CHUNKS, cores + lines)),
        dma((ROW_CHUNKS, n_tp)),
        dma((ROW_CHUNKS, ol, oc)),
        dma((n_tp,)),
        dma(()),
    ]
    in_specs = [pl.BlockSpec(memory_space=pltpu.VMEM)] * 9 + [pl.BlockSpec(memory_space=pl.ANY)] * 9
    return pl.pallas_call(
        kernel,
        out_shape=jax.ShapeDtypeStruct((own, width), BF16),
        in_specs=in_specs,
        out_specs=pl.BlockSpec(memory_space=pltpu.VMEM),
        scratch_shapes=scratch,
        compiler_params=pltpu.CompilerParams(
            collective_id=0, has_side_effects=True, vmem_limit_bytes=67_000_000
        ),
    )


def shards(
    query_proj, key_proj, value_proj, gate_proj, log_decay, residual, out_weight, norm_gain,
    norm_bias, up_gate, up_value, conv_weight, conv_bias, down_weight,
):
    n_sp, n_tp = lax.axis_size("sp"), lax.axis_size("tp")
    tok_rows, heads = log_decay.shape
    key_width = query_proj.shape[1] // heads
    value_width = value_proj.shape[1] // heads
    nb = tok_rows // BLOCK
    call = make_kernel(
        n_sp, n_tp, tok_rows, heads, key_width, value_width,
        residual.shape[1], up_gate.shape[0], up_gate.shape[1],
    )
    tables = rotary_tables(key_width, n_sp * nb)
    logs = log_decay.T.reshape(heads * nb, BLOCK)
    return call(
        *tables, logs, norm_gain, norm_bias, conv_weight, conv_bias, query_proj, key_proj,
        value_proj, gate_proj, residual, out_weight, up_gate, up_value, down_weight,
    )


def solution(mesh):
    placed = (
        P("sp", "tp"), P("sp", "tp"), P("sp", "tp"), P("sp", "tp"), P("sp", "tp"),
        P("sp", None), P("tp", None), P(), P(), P("sp", "tp"), P("sp", "tp"),
        P(None, None, "tp"), P(None, "tp"), P("tp", "sp"),
    )
    return jax.shard_map(
        shards, mesh=mesh, in_specs=placed, out_specs=P(("sp", "tp"), None), check_vma=False
    )
```

```python
import numpy as np
import jax
import jax.numpy as jnp
from jax import lax
from jax.experimental import pallas as pl
from jax.experimental.pallas import tpu as pltpu
from jax.sharding import PartitionSpec as P

BLOCK = 256
HALO = 16
ROW_CHUNKS = 4

alpha_scale = 8.0**0.25
rope_base = 10000.0
tiny_stabilizer = 1e-05
MESH = pl.DeviceIdType.MESH
F32, BF16 = jnp.float32, jnp.bfloat16


def dot(a, b):
    return jnp.dot(a, b, preferred_element_type=F32)


def dot_t(a, b, dims, precision=None):
    return lax.dot_general(a, b, (dims, ((), ())), precision=precision, preferred_element_type=F32)


def layout(sp, tp):
    cores = 2 if tp % 2 == 0 else 1
    lines = tp // cores
    ny = lines if sp % lines == 0 else 1
    return cores, lines, ny, sp // ny


def rotary_tables(head_width, blocks):
    half = head_width // 2
    freq = rope_base ** (-2.0 * np.arange(half, dtype=np.float64) / head_width)
    inner = np.arange(BLOCK, dtype=np.float64)[:, None] * freq
    outer = (np.arange(blocks, dtype=np.float64) * BLOCK)[:, None] * freq
    tables = (np.cos(inner), np.sin(inner), np.cos(outer), np.sin(outer))
    return [jnp.asarray(t.astype(np.float32)) for t in tables]


class Sends:
    def __init__(self):
        self.left = []

    def start(self, copy, cond=None):
        self.left.append((copy, cond))
        if cond is None:
            copy.start()
        else:
            pl.when(cond)(copy.start)

    def drain(self):
        for copy, cond in self.left:
            if cond is None:
                copy.wait_send()
            else:
                pl.when(cond)(copy.wait_send)
        self.left = []


def make_kernel(n_sp, n_tp, tok_rows, heads, key_width, value_width, width, depth, hidden):
    cores, lines, ny, nz = layout(n_sp, n_tp)
    nb = tok_rows // BLOCK
    own = tok_rows // n_tp
    piece = width // n_sp
    slice_w = value_width // ny
    half_k = key_width // 2
    dh, hh = depth // 2, hidden // 2
    chunk = own // ROW_CHUNKS
    hcols = 128 if hidden % 128 == 0 else hidden

    def kernel(
        cos_in, sin_in, cos_out, sin_out, log_ref, gain, bias, taps, shift,
        q_hbm, k_hbm, v_hbm, g_hbm, res_hbm, ow_hbm, upg, upv, down,
        out,
        wg, wd, qb, kb, vb, gb, ow, res, cum_col, st, lb, within,
        xs, xr, dec, chain_s, chain_r, cb, cs, part, r1, s2, r2, acc, rows, ups, act,
        load_sem, bulk_r, bulk_z, bulk_y, st_s, st_r, dec_s, dec_r, ch_s, ch_r, cb_s, cb_r,
        rs1_s, rs1_r, rs2_s, rs2_r, ag_s, ag_r, agf_s, halo_s, halo_r,
    ):
        sp, tp = lax.axis_index("sp"), lax.axis_index("tp")
        z, y = sp // ny, sp % ny
        x, c = tp // cores, tp % cores
        me_sp = sp

        def remote(src, dst, ssem, rsem, to_sp, to_tp):
            return pltpu.make_async_remote_copy(
                src_ref=src, dst_ref=dst, send_sem=ssem, recv_sem=rsem,
                device_id=(to_sp, to_tp), device_id_type=MESH,
            )

        def arrived(dst, ssem, rsem, cond=None):
            copy = remote(dst, dst, ssem, rsem, sp, tp)
            if cond is None:
                copy.wait_recv()
            else:
                pl.when(cond)(copy.wait_recv)

        own_rows = pl.ds(pl.multiple_of(tp * own, own), own)
        pairs = [
            (k_hbm, kb), (v_hbm, vb), (q_hbm, qb), (g_hbm, gb), (ow_hbm, ow),
            (res_hbm.at[own_rows], res), (upg, wg.at[me_sp, 0]), (upv, wg.at[me_sp, 1]),
            (down, wd.at[me_sp]),
        ]
        loads = [pltpu.make_async_copy(a, b, load_sem.at[i]) for i, (a, b) in enumerate(pairs)]
        for load in loads:
            load.start()

        barrier = pltpu.get_barrier_semaphore()

        def greet(to_sp, to_tp, cond=None):
            def go():
                pl.semaphore_signal(barrier, inc=1, device_id=(to_sp, to_tp), device_id_type=MESH)

            if cond is None:
                go()
            else:
                pl.when(cond)(go)

        other_y = [z * ny + (y + d) % ny for d in range(1, ny)]
        other_c = [x * cores + (c + d) % cores for d in range(1, cores)]
        other_x = [(x + d) % lines * cores + c for d in range(1, lines)]
        peers = [(sp + ny, tp, z < nz - 1), (sp - ny, tp, z > 0)]
        peers += [(o, tp, None) for o in other_y]
        peers += [(sp, o, None) for o in other_c + other_x]
        for t in range(n_tp):
            peers.append((sp + 1, t, jnp.logical_and(tp == n_tp - 1, sp < n_sp - 1)))
        for to_sp, to_tp, cond in peers:
            greet(to_sp, to_tp, cond)
        greet(sp - 1, n_tp - 1, sp > 0)
        count = (sp > 0).astype(jnp.int32)
        for _, _, cond in peers:
            count = count + (1 if cond is None else cond.astype(jnp.int32))
        pl.semaphore_wait(barrier, count)

        bulk = Sends()

        def slot(p, src):
            m, h = p // 2, p % 2
            if m < 2:
                return wg.at[src, m, pl.ds(h * dh, dh)]
            return wd.at[src, pl.ds(h * hh, hh)]

        def mine(p):
            m, h = p // 2, p % 2
            if m == 2:
                return down.at[pl.ds(h * hh, hh)]
            return (upg, upv)[m].at[pl.ds(h * dh, dh)]

        def own_z(p, up, also=None):
            cond, to = (z < nz - 1, sp + ny) if up else (z > 0, sp - ny)
            if also is not None:
                cond = jnp.logical_and(cond, also)
            bulk.start(
                remote(mine(p), slot(p, sp), bulk_z.at[p, 0 if up else 1], bulk_r.at[p, sp], to, tp),
                cond,
            )

        def own_y(p):
            for d, to in enumerate(other_y):
                bulk.start(
                    remote(mine(p), slot(p, sp), bulk_y.at[p, 0, d], bulk_r.at[p, sp], to, tp)
                )

        middle = jnp.logical_and(z > 0, z < nz - 1)

        def source(up, d, also=None):
            src, cond = (sp - d * ny, z >= d) if up else (sp + d * ny, z < nz - d)
            return src, cond if also is None else jnp.logical_and(cond, also)

        def take(p, up, d, also=None):
            src, cond = source(up, d, also)
            src = jnp.clip(src, 0, n_sp - 1)
            arrived(slot(p, src), bulk_z.at[p, 0], bulk_r.at[p, src], cond)

        def on_z(p, up, d, also=None):
            src, cond = source(up, d, also)
            src = jnp.clip(src, 0, n_sp - 1)
            to, more = (sp + ny, z < nz - 1) if up else (sp - ny, z > 0)
            sem = bulk_z.at[p, 2 * d + (0 if up else 1)]
            bulk.start(
                remote(slot(p, src), slot(p, src), sem, bulk_r.at[p, src], to, tp),
                jnp.logical_and(cond, more),
            )

        balanced = ny == 2 and nz >= 4

        def by_y(p, src_z):
            if not balanced:
                return jnp.bool_(True)
            m, h = p // 2, p % 2
            skip = jnp.logical_or(
                jnp.logical_and(z == 1, src_z == 0),
                jnp.logical_and(z == nz - 2, src_z == nz - 1),
            )
            if m == 2 or h == 1:
                skip = jnp.logical_or(skip, jnp.logical_and(z == 0, src_z == 1))
            if h == 1:
                skip = jnp.logical_or(skip, jnp.logical_and(z == nz - 1, src_z == nz - 2))
            return jnp.logical_not(skip)

        def beside(p):
            m, h = p // 2, p % 2
            src = z * ny + (y + 1) % ny
            arrived(slot(p, src), bulk_z.at[p, 0], bulk_r.at[p, src])
            cond = jnp.logical_or(z == 0, z == nz - 1)
            if h == 1:
                cond = jnp.logical_or(cond, jnp.logical_or(z == 1, z == nz - 2))
            elif m == 2:
                cond = jnp.logical_or(cond, z == 1)
            down_to = jnp.logical_or(z == 1, z == nz - 1)
            to = jnp.where(down_to, z - 1, z + 1) * ny + y
            bulk.start(
                remote(slot(p, src), slot(p, src), bulk_z.at[p, 2 * nz], bulk_r.at[p, src], to, tp),
                cond,
            )

        def share(m):
            if balanced:
                beside(2 * m)
                beside(2 * m + 1)

        def on_y(p, up, d, also=None):
            src, cond = source(up, d, also)
            cond = jnp.logical_and(cond, by_y(p, src // ny))
            src = jnp.clip(src, 0, n_sp - 1)
            for e, to in enumerate(other_y):
                sem = bulk_y.at[p, 2 * d + (0 if up else 1), e]
                bulk.start(
                    remote(slot(p, src), slot(p, src), sem, bulk_r.at[p, src], to, tp), cond
                )

        def relay(m, up, d, also=None):
            if d >= nz:
                return
            for p in (2 * m, 2 * m + 1):
                take(p, up, d, also)
                if d < nz - 1:
                    on_z(p, up, d, also)
                on_y(p, up, d, also)

        def side_arrivals(m):
            for src in range(n_sp):
                for p in (2 * m, 2 * m + 1):
                    cond = src % ny != y
                    if balanced:
                        cond = jnp.logical_and(cond, src // ny != z)
                    arrived(slot(p, src), bulk_z.at[p, 0], bulk_r.at[p, src], cond)

        own_z(0, True)
        own_z(1, True, z > 0)
        for p in (0, 1, 2, 3):
            own_z(p, False)

        ii = lax.broadcasted_iota(jnp.int32, (BLOCK, BLOCK), 0)
        jj = lax.broadcasted_iota(jnp.int32, (BLOCK, BLOCK), 1)
        lower = (ii >= jj).astype(F32)
        logs = log_ref[...]
        cum_col[...] = dot_t(lower, logs, ((1,), (1,)), lax.Precision.HIGHEST)

        def column(idx):
            lane = lax.broadcasted_iota(jnp.int32, cum_col.shape, 1)
            return jnp.sum(jnp.where(lane == idx, cum_col[...], 0.0), axis=1, keepdims=True)

        def angles(b):
            row = pl.ds(sp * nb + b, 1)
            co, so = cos_out[row, :], sin_out[row, :]
            ci, si = cos_in[...], sin_in[...]
            return ci * co - si * so, si * co + ci * so

        def rotated(value, cosine, sine):
            front, second = value[:, :half_k], value[:, half_k:]
            return jnp.concatenate(
                [front * cosine - second * sine, front * sine + second * cosine], axis=1
            )

        def block_rows(b):
            return pl.ds(pl.multiple_of(b * BLOCK, BLOCK), BLOCK)

        loads[0].wait()
        loads[1].wait()
        st[...] = jnp.zeros_like(st)

        def local_states(b, _):
            r = block_rows(b)
            cosine, sine = angles(b)
            for h in range(heads):
                cc = column(h * nb + b)
                total = cc[BLOCK - 1 : BLOCK, :]
                kc = pl.ds(h * key_width, key_width)
                key = rotated(kb[r, kc].astype(F32), cosine, sine) * key_width ** (-0.5)
                key = key.astype(BF16)
                kb[r, kc] = key
                faded = (key.astype(F32) * jnp.exp(total - cc)).astype(BF16)
                term = dot_t(faded, vb[r, pl.ds(h * value_width, value_width)], ((0,), (0,)))
                before = st[h]
                lb[b * heads + h] = before.astype(BF16)
                st[h] = jnp.exp(total) * before + term
            return 0

        lax.fori_loop(0, nb, local_states, 0)

        def head_log(h):
            total = jnp.zeros((1, 1), F32)
            for b in range(nb):
                total = total + jnp.sum(logs[h * nb + b : h * nb + b + 1, :], axis=1, keepdims=True)
            return total

        hrow = lax.broadcasted_iota(jnp.int32, (8, 128), 0)
        tile = jnp.zeros((8, 128), F32)
        for h in range(heads):
            tile = jnp.where(hrow == h, head_log(h), tile)
        dec[pl.ds(y, 1)] = tile[None]
        states = Sends()
        for d, to in enumerate(other_y):
            far = (y + d + 1) % ny
            states.start(
                remote(dec.at[y], dec.at[y], dec_s.at[d], dec_r.at[y], to, tp)
            )
            for h in range(heads):
                for f in range(ny):

                    @pl.when(far == f)
                    def _():
                        xs[d, h] = st[h, :, f * slice_w : (f + 1) * slice_w].astype(BF16)

                states.start(
                    remote(xs.at[d, h], xr.at[y, h], st_s.at[d, h], st_r.at[y, h], to, tp)
                )
        own_y(0)
        own_y(1)

        loads[2].wait()

        def within_block(b, _):
            r = block_rows(b)
            cosine, sine = angles(b)
            for h in range(heads):
                cc = column(h * nb + b)
                kc = pl.ds(h * key_width, key_width)
                query = rotated(qb[r, kc].astype(F32), cosine, sine).astype(BF16)
                scores = dot_t(query, kb[r, kc], ((1,), (1,)))
                crow = jnp.sum(jnp.where(ii == jj, cc, 0.0), axis=0, keepdims=True)
                gap = jnp.where(ii >= jj, cc - crow, 0.0)
                weight = jnp.where(ii >= jj, jnp.exp(gap), 0.0)
                vc = pl.ds(h * value_width, value_width)
                within[r, vc] = dot((scores * weight).astype(BF16), vb[r, vc])
                qb[r, kc] = (query.astype(F32) * jnp.exp(cc)).astype(BF16)
            return 0

        lax.fori_loop(0, nb, within_block, 0)

        for f in range(ny):

            @pl.when(y == f)
            def _():
                for h in range(heads):
                    xr[f, h] = st[h, :, f * slice_w : (f + 1) * slice_w].astype(BF16)

        for d in range(1, ny):
            src = (y + d) % ny
            arrived(dec.at[src], dec_s.at[0], dec_r.at[src])
            for h in range(heads):
                arrived(xr.at[src, h], st_s.at[0, 0], st_r.at[src, h])
        for h in range(heads):

            @pl.when(z == 0)
            def _():
                chain_r[h] = jnp.zeros((key_width, slice_w), BF16)

            arrived(chain_r.at[h], ch_s.at[h], ch_r.at[h], z > 0)
            incoming = chain_r[h].astype(F32)
            before = incoming
            for f in range(ny):
                cb_mine = before.astype(BF16)

                @pl.when(y == f)
                def _():
                    cb[y, h] = cb_mine

                @pl.when(y != f)
                def _():
                    cs[f, h] = cb_mine

                decay = jnp.exp(dec[f, h : h + 1, 0:1])
                before = decay * before + xr[f, h].astype(F32)
            chain_s[h] = before.astype(BF16)
            states.start(
                remote(chain_s.at[h], chain_r.at[h], ch_s.at[h], ch_r.at[h], sp + ny, tp),
                z < nz - 1,
            )
            for d, to in enumerate(other_y):
                far = (y + d + 1) % ny
                states.start(
                    remote(cs.at[far, h], cb.at[y, h], cb_s.at[d, h], cb_r.at[y, h], to, tp)
                )

        own_z(1, True, z == 0)
        for p in (2, 3):
            own_z(p, True)
            own_y(p)
        relay(0, False, 1)
        share(0)

        loads[3].wait()
        for h in range(heads):
            for d in range(1, ny):
                src = (y + d) % ny
                arrived(cb.at[src, h], cb_s.at[0, 0], cb_r.at[src, h])

            def finish(b, decay):
                r = block_rows(b)
                vc = pl.ds(h * value_width, value_width)
                state = jnp.concatenate([cb[f, h].astype(F32) for f in range(ny)], axis=1)
                state = (decay * state + lb[b * heads + h].astype(F32)).astype(BF16)
                mixed = within[r, vc] + dot(qb[r, pl.ds(h * key_width, key_width)], state)
                average = jnp.mean(mixed, axis=1, keepdims=True)
                mixed = mixed - average
                spread = jnp.mean(mixed * mixed, axis=1, keepdims=True)
                gate = gb[r, vc].astype(F32)
                gated = gate * jax.nn.sigmoid(gate) * (mixed * lax.rsqrt(spread + tiny_stabilizer))
                gb[r, vc] = gated.astype(BF16)
                return decay * jnp.exp(column(h * nb + b)[BLOCK - 1 : BLOCK, :])

            lax.fori_loop(0, nb, finish, jnp.ones((1, 1), F32))
        states.drain()
        relay(0, True, 1)

        def owner_rows(xx, cc):
            return pl.ds(pl.multiple_of((xx * cores + cc) * own, own), own)

        def piece_cols(s):
            return pl.ds(pl.multiple_of(s * piece, piece), piece)

        def d2d_copies(s):
            return [
                remote(
                    part.at[s, owner_rows(xx, (c + d) % cores)], r1.at[s, d - 1, xx],
                    rs1_s.at[s, d - 1, xx], rs1_r.at[s, d - 1, xx],
                    sp, x * cores + (c + d) % cores,
                )
                for d in range(1, cores)
                for xx in range(lines)
            ]

        def x_copies(s):
            return [
                remote(
                    s2.at[s, d - 1], r2.at[s, d - 1], rs2_s.at[s, d - 1], rs2_r.at[s, d - 1],
                    sp, (x + d) % lines * cores + c,
                )
                for d in range(1, lines)
            ]

        row_tile = min(tok_rows, 512)

        def product(s, lhs, rhs):
            def one(i, _):
                r = pl.ds(pl.multiple_of(i * row_tile, row_tile), row_tile)
                part[s, r, :] = dot(lhs[r, :], rhs()).astype(BF16)
                return 0

            lax.fori_loop(0, tok_rows // row_tile, one, 0)
            for copy in d2d_copies(s):
                copy.start()

        def combine(s):
            for copy in d2d_copies(s):
                copy.wait_recv()
            for d in range(lines):
                xx = (x + d) % lines
                total = part[s, owner_rows(xx, c), :].astype(F32)
                for e in range(cores - 1):
                    total = total + r1[s, e, xx].astype(F32)
                if d == 0:
                    acc[:, piece_cols(s)] = total
                else:
                    s2[s, d - 1] = total.astype(BF16)
            for copy in x_copies(s):
                copy.start()

        def collect(s):
            for copy in x_copies(s):
                copy.wait_recv()
            total = acc[:, piece_cols(s)]
            for d in range(lines - 1):
                total = total + r2[s, d].astype(F32)
            acc[:, piece_cols(s)] = total

        def release(s, _):
            for copy in d2d_copies(s) + x_copies(s):
                copy.wait_send()
            return 0

        def out_step(s, _):
            product(s, gb, lambda: ow[:, piece_cols(s)])
            pl.when(s > 0)(lambda: combine(s - 1))
            return 0

        loads[4].wait()
        lax.fori_loop(0, n_sp, out_step, 0)
        combine(n_sp - 1)
        relay(0, False, 2)
        relay(0, True, 2)
        relay(1, False, 1)
        relay(1, True, 1)

        def collect_step(s, _):
            collect(s)
            return 0

        lax.fori_loop(0, n_sp, collect_step, 0)

        loads[5].wait()

        def layer_norm(values, which):
            average = jnp.mean(values, axis=1, keepdims=True)
            values = values - average
            spread = jnp.mean(values * values, axis=1, keepdims=True)
            values = values * lax.rsqrt(spread + tiny_stabilizer)
            return values * gain[which : which + 1, :] + bias[which : which + 1, :]

        ln_rows = 32
        gathered = Sends()

        def chunk_of(owner, j):
            return rows.at[pl.ds(pl.multiple_of(HALO + owner * own + j * chunk, 16), chunk)]

        pl.when(sp == 0)(lambda: rows.__setitem__((pl.ds(0, HALO), slice(None)), jnp.zeros((HALO, width), BF16)))
        for j in range(ROW_CHUNKS):

            def norm_rows(i, _):
                at = pl.multiple_of(j * chunk + i * ln_rows, ln_rows)
                r = pl.ds(at, ln_rows)
                value = layer_norm(alpha_scale * res[r, :].astype(F32) + acc[r, :], 0).astype(BF16)
                res[r, :] = value
                rows[pl.ds(pl.multiple_of(HALO + tp * own + at, 16), ln_rows), :] = value
                return 0

            lax.fori_loop(0, chunk // ln_rows, norm_rows, 0)
            for d, to in enumerate(other_c + other_x):
                gathered.start(
                    remote(chunk_of(tp, j), chunk_of(tp, j), ag_s.at[j, d], ag_r.at[j, tp], sp, to)
                )
        last = pl.ds(tok_rows, HALO)
        for t in range(n_tp):
            gathered.start(
                remote(rows.at[last], rows.at[pl.ds(0, HALO)], halo_s.at[t], halo_r, sp + 1, t),
                jnp.logical_and(tp == n_tp - 1, sp < n_sp - 1),
            )
        for j in range(ROW_CHUNKS):
            if j == ROW_CHUNKS // 2:
                relay(0, False, 3)
                relay(1, False, 2, z > 0)
                relay(1, True, 2, z < nz - 1)
                share(1)
            if j == ROW_CHUNKS - 1:
                relay(0, True, 3)
            for d in range(1, lines):
                owner = (x + d) % lines * cores + c
                arrived(chunk_of(owner, j), ag_s.at[j, 0], ag_r.at[j, owner])
                for e, to in enumerate(other_c):
                    gathered.start(
                        remote(
                            chunk_of(owner, j), chunk_of(owner, j),
                            agf_s.at[j, d - 1, e], ag_r.at[j, owner], sp, to,
                        )
                    )
        for d in range(1, cores):
            for e in range(lines):
                owner = (x + e) % lines * cores + (c + d) % cores
                for j in range(ROW_CHUNKS):
                    arrived(chunk_of(owner, j), ag_s.at[j, 0], ag_r.at[j, owner])
        for p in (4, 5):
            own_z(p, False)
            own_z(p, True)
        relay(1, False, 2, z == 0)
        relay(1, True, 2, z == nz - 1)
        for d in range(4, nz):
            relay(0, False, d)
            relay(0, True, d)
        lax.fori_loop(0, n_sp, release, 0)

        def up_tile(m, start, count):
            r = pl.ds(start, count)
            total = None
            for s in range(n_sp):
                term = dot(rows[r, s * depth : (s + 1) * depth], wg[s, m])
                total = term if total is None else total + term
            ups[m, r, :] = total.astype(BF16)

        def up_rows(m):
            def one(i, _):
                up_tile(m, pl.multiple_of(HALO + i * BLOCK, 16), BLOCK)
                return 0

            lax.fori_loop(0, tok_rows // BLOCK, one, 0)
            up_tile(m, 0, HALO)

        loads[6].wait()
        side_arrivals(0)
        arrived(rows.at[pl.ds(0, HALO)], halo_s.at[0], halo_r, sp > 0)
        up_rows(0)
        for d in range(3, nz):
            relay(1, False, d)
            relay(1, True, d)
        own_y(4)
        own_y(5)
        relay(2, False, 1, middle)
        relay(2, True, 1, middle)
        loads[7].wait()
        side_arrivals(1)
        up_rows(1)

        def activate(i, col):
            at = pl.multiple_of(i * BLOCK, BLOCK)
            convs = []
            for m in range(2):
                tile = ups[m, pl.ds(at, BLOCK + HALO), col].astype(F32)
                value = shift[m : m + 1, col]
                for j in range(3):
                    value = value + taps[m, j : j + 1, col] * tile[HALO - 2 + j : HALO - 2 + j + BLOCK, :]
                convs.append(value)
            act[pl.ds(at, BLOCK), col] = (jax.nn.gelu(convs[0]) * convs[1]).astype(BF16)

        def activate_step(i, _):
            for t in range(hidden // hcols):
                activate(i, pl.ds(t * hcols, hcols))
            return 0

        lax.fori_loop(0, tok_rows // BLOCK, activate_step, 0)

        order = [
            [zz] + sorted((o for o in range(nz) if o != zz), key=lambda o: (abs(o - zz), abs(2 * o - nz + 1)))
            for zz in range(nz)
        ]

        def nearest(k):
            got = jnp.int32(order[0][k])
            for zz in range(1, nz):
                got = jnp.where(z == zz, order[zz][k], got)
            return got

        first = [(k, 0) for k in range(nz)]
        second = [(k, d) for k in range(nz) for d in range(1, ny)]
        steps = first[:-1] + second[: ny - 1] + first[-1:] + second[ny - 1 :]
        loads[8].wait()
        previous = None
        done = []
        for k, d in steps:
            src_z = nearest(k)
            src = src_z * ny + (y + d) % ny
            if balanced and d > 0 and k == 0:
                share(2)
            elif d > 0:
                for p in (4, 5):
                    arrived(slot(p, src), bulk_z.at[p, 0], bulk_r.at[p, src])
            elif k > 0:
                to_z = jnp.where(src_z < z, z + 1, z - 1)
                more = jnp.logical_and(to_z >= 0, to_z < nz)
                fresh = jnp.logical_not(jnp.logical_and(middle, jnp.abs(src_z - z) == 1))
                for p in (4, 5):
                    arrived(slot(p, src), bulk_z.at[p, 0], bulk_r.at[p, src], fresh)
                    bulk.start(
                        remote(
                            slot(p, src), slot(p, src), bulk_z.at[p, 2 * nz + k],
                            bulk_r.at[p, src], to_z * ny + y, tp,
                        ),
                        jnp.logical_and(more, fresh),
                    )
                    for e, to in enumerate(other_y):
                        bulk.start(
                            remote(
                                slot(p, src), slot(p, src), bulk_y.at[p, 2 * nz + k, e],
                                bulk_r.at[p, src], to, tp,
                            ),
                            jnp.logical_and(by_y(p, src_z), fresh),
                        )
            product(src, act, lambda: wd[src])
            if previous is not None:
                combine(previous)
            previous = src
            done.append(src)
        combine(previous)
        for src in done:
            collect(src)

        def final_rows(i, _):
            r = pl.ds(pl.multiple_of(i * ln_rows, ln_rows), ln_rows)
            out[r, :] = layer_norm(alpha_scale * res[r, :].astype(F32) + acc[r, :], 1).astype(BF16)
            return 0

        lax.fori_loop(0, own // ln_rows, final_rows, 0)
        lax.fori_loop(0, n_sp, release, 0)
        gathered.drain()
        bulk.drain()

    vmem, dma = pltpu.VMEM, pltpu.SemaphoreType.DMA
    oc, ol, oy = max(cores - 1, 1), max(lines - 1, 1), max(ny - 1, 1)
    scratch = [
        vmem((n_sp, 2, depth, hidden), BF16),
        vmem((n_sp, hidden, piece), BF16),
        vmem((tok_rows, heads * key_width), BF16),
        vmem((tok_rows, heads * key_width), BF16),
        vmem((tok_rows, heads * value_width), BF16),
        vmem((tok_rows, heads * value_width), BF16),
        vmem((heads * value_width, width), BF16),
        vmem((own, width), BF16),
        vmem((BLOCK, heads * nb), F32),
        vmem((heads, key_width, value_width), F32),
        vmem((nb * heads, key_width, value_width), BF16),
        vmem((tok_rows, heads * value_width), F32),
        vmem((oy, heads, key_width, slice_w), BF16),
        vmem((ny, heads, key_width, slice_w), BF16),
        vmem((ny, 8, 128), F32),
        vmem((heads, key_width, slice_w), BF16),
        vmem((heads, key_width, slice_w), BF16),
        vmem((ny, heads, key_width, slice_w), BF16),
        vmem((ny, heads, key_width, slice_w), BF16),
        vmem((n_sp, tok_rows, piece), BF16),
        vmem((n_sp, oc, lines, own, piece), BF16),
        vmem((n_sp, ol, own, piece), BF16),
        vmem((n_sp, ol, own, piece), BF16),
        vmem((own, width), F32),
        vmem((HALO + tok_rows, width), BF16),
        vmem((2, HALO + tok_rows, hidden), BF16),
        vmem((tok_rows, hidden), BF16),
        dma((9,)),
        dma((6, n_sp)),
        dma((6, 3 * nz)),
        dma((6, 3 * nz, oy)),
        dma((oy, heads)),
        dma((ny, heads)),
        dma((oy,)),
        dma((ny,)),
        dma((heads,)),
        dma((heads,)),
        dma((oy, heads)),
        dma((ny, heads)),
        dma((n_sp, oc, lines)),
        dma((n_sp, oc, lines)),
        dma((n_sp, ol)),
        dma((n_sp, ol)),
        dma((ROW_CHUNKS, cores + lines)),
        dma((ROW_CHUNKS, n_tp)),
        dma((ROW_CHUNKS, ol, oc)),
        dma((n_tp,)),
        dma(()),
    ]
    in_specs = [pl.BlockSpec(memory_space=pltpu.VMEM)] * 9 + [pl.BlockSpec(memory_space=pl.ANY)] * 9
    return pl.pallas_call(
        kernel,
        out_shape=jax.ShapeDtypeStruct((own, width), BF16),
        in_specs=in_specs,
        out_specs=pl.BlockSpec(memory_space=pltpu.VMEM),
        scratch_shapes=scratch,
        compiler_params=pltpu.CompilerParams(
            collective_id=0, has_side_effects=True, vmem_limit_bytes=67_000_000
        ),
    )


def shards(
    query_proj, key_proj, value_proj, gate_proj, log_decay, residual, out_weight, norm_gain,
    norm_bias, up_gate, up_value, conv_weight, conv_bias, down_weight,
):
    n_sp, n_tp = lax.axis_size("sp"), lax.axis_size("tp")
    tok_rows, heads = log_decay.shape
    key_width = query_proj.shape[1] // heads
    value_width = value_proj.shape[1] // heads
    nb = tok_rows // BLOCK
    call = make_kernel(
        n_sp, n_tp, tok_rows, heads, key_width, value_width,
        residual.shape[1], up_gate.shape[0], up_gate.shape[1],
    )
    tables = rotary_tables(key_width, n_sp * nb)
    logs = log_decay.T.reshape(heads * nb, BLOCK)
    return call(
        *tables, logs, norm_gain, norm_bias, conv_weight, conv_bias, query_proj, key_proj,
        value_proj, gate_proj, residual, out_weight, up_gate, up_value, down_weight,
    )


def solution(mesh):
    placed = (
        P("sp", "tp"), P("sp", "tp"), P("sp", "tp"), P("sp", "tp"), P("sp", "tp"),
        P("sp", None), P("tp", None), P(), P(), P("sp", "tp"), P("sp", "tp"),
        P(None, None, "tp"), P(None, "tp"), P("tp", "sp"),
    )
    return jax.shard_map(
        shards, mesh=mesh, in_specs=placed, out_specs=P(("sp", "tp"), None), check_vma=False
    )
```

```python
import numpy as np
import jax
import jax.numpy as jnp
from jax import lax
from jax.experimental import pallas as pl
from jax.experimental.pallas import tpu as pltpu
from jax.sharding import PartitionSpec as P

BLOCK = 256
HALO = 16
ROW_CHUNKS = 4

alpha_scale = 8.0**0.25
rope_base = 10000.0
tiny_stabilizer = 1e-05
MESH = pl.DeviceIdType.MESH
F32, BF16 = jnp.float32, jnp.bfloat16


def dot(a, b):
    return jnp.dot(a, b, preferred_element_type=F32)


def dot_t(a, b, dims, precision=None):
    return lax.dot_general(a, b, (dims, ((), ())), precision=precision, preferred_element_type=F32)


def layout(sp, tp):
    cores = 2 if tp % 2 == 0 else 1
    lines = tp // cores
    ny = lines if sp % lines == 0 else 1
    return cores, lines, ny, sp // ny


def rotary_tables(head_width, blocks):
    half = head_width // 2
    freq = rope_base ** (-2.0 * np.arange(half, dtype=np.float64) / head_width)
    inner = np.arange(BLOCK, dtype=np.float64)[:, None] * freq
    outer = (np.arange(blocks, dtype=np.float64) * BLOCK)[:, None] * freq
    tables = (np.cos(inner), np.sin(inner), np.cos(outer), np.sin(outer))
    return [jnp.asarray(t.astype(np.float32)) for t in tables]


class Sends:
    def __init__(self):
        self.left = []

    def start(self, copy, cond=None):
        self.left.append((copy, cond))
        if cond is None:
            copy.start()
        else:
            pl.when(cond)(copy.start)

    def drain(self):
        for copy, cond in self.left:
            if cond is None:
                copy.wait_send()
            else:
                pl.when(cond)(copy.wait_send)
        self.left = []


def make_kernel(n_sp, n_tp, tok_rows, heads, key_width, value_width, width, depth, hidden):
    cores, lines, ny, nz = layout(n_sp, n_tp)
    nb = tok_rows // BLOCK
    own = tok_rows // n_tp
    piece = width // n_sp
    slice_w = value_width // ny
    half_k = key_width // 2
    dh, hh = depth // 2, hidden // 2
    chunk = own // ROW_CHUNKS
    hcols = 128 if hidden % 128 == 0 else hidden

    def kernel(
        cos_in, sin_in, cos_out, sin_out, log_ref, gain, bias, taps, shift,
        q_hbm, k_hbm, v_hbm, g_hbm, res_hbm, ow_hbm, upg, upv, down,
        out,
        wg, wd, qb, kb, vb, gb, ow, res, cum_col, st, lb, within,
        xs, xr, dec, chain_s, chain_r, cb, cs, part, r1, s2, r2, acc, rows, ups, act,
        load_sem, bulk_r, bulk_z, bulk_y, st_s, st_r, dec_s, dec_r, ch_s, ch_r, cb_s, cb_r,
        rs1_s, rs1_r, rs2_s, rs2_r, ag_s, ag_r, agf_s, halo_s, halo_r,
    ):
        sp, tp = lax.axis_index("sp"), lax.axis_index("tp")
        z, y = sp // ny, sp % ny
        x, c = tp // cores, tp % cores
        me_sp = sp

        def remote(src, dst, ssem, rsem, to_sp, to_tp):
            return pltpu.make_async_remote_copy(
                src_ref=src, dst_ref=dst, send_sem=ssem, recv_sem=rsem,
                device_id=(to_sp, to_tp), device_id_type=MESH,
            )

        def arrived(dst, ssem, rsem, cond=None):
            copy = remote(dst, dst, ssem, rsem, sp, tp)
            if cond is None:
                copy.wait_recv()
            else:
                pl.when(cond)(copy.wait_recv)

        own_rows = pl.ds(pl.multiple_of(tp * own, own), own)
        pairs = [
            (k_hbm, kb), (v_hbm, vb), (q_hbm, qb), (g_hbm, gb), (ow_hbm, ow),
            (res_hbm.at[own_rows], res), (upg, wg.at[me_sp, 0]), (upv, wg.at[me_sp, 1]),
            (down, wd.at[me_sp]),
        ]
        loads = [pltpu.make_async_copy(a, b, load_sem.at[i]) for i, (a, b) in enumerate(pairs)]
        for load in loads:
            load.start()

        barrier = pltpu.get_barrier_semaphore()

        def greet(to_sp, to_tp, cond=None):
            def go():
                pl.semaphore_signal(barrier, inc=1, device_id=(to_sp, to_tp), device_id_type=MESH)

            if cond is None:
                go()
            else:
                pl.when(cond)(go)

        other_y = [z * ny + (y + d) % ny for d in range(1, ny)]
        other_c = [x * cores + (c + d) % cores for d in range(1, cores)]
        other_x = [(x + d) % lines * cores + c for d in range(1, lines)]
        peers = [(sp + ny, tp, z < nz - 1), (sp - ny, tp, z > 0)]
        peers += [(o, tp, None) for o in other_y]
        peers += [(sp, o, None) for o in other_c + other_x]
        for t in range(n_tp):
            peers.append((sp + 1, t, jnp.logical_and(tp == n_tp - 1, sp < n_sp - 1)))
        for to_sp, to_tp, cond in peers:
            greet(to_sp, to_tp, cond)
        greet(sp - 1, n_tp - 1, sp > 0)
        count = (sp > 0).astype(jnp.int32)
        for _, _, cond in peers:
            count = count + (1 if cond is None else cond.astype(jnp.int32))
        pl.semaphore_wait(barrier, count)

        bulk = Sends()

        def slot(p, src):
            m, h = p // 2, p % 2
            if m < 2:
                return wg.at[src, m, pl.ds(h * dh, dh)]
            return wd.at[src, pl.ds(h * hh, hh)]

        def mine(p):
            m, h = p // 2, p % 2
            if m == 2:
                return down.at[pl.ds(h * hh, hh)]
            return (upg, upv)[m].at[pl.ds(h * dh, dh)]

        def own_z(p, up, also=None):
            cond, to = (z < nz - 1, sp + ny) if up else (z > 0, sp - ny)
            if also is not None:
                cond = jnp.logical_and(cond, also)
            bulk.start(
                remote(mine(p), slot(p, sp), bulk_z.at[p, 0 if up else 1], bulk_r.at[p, sp], to, tp),
                cond,
            )

        def own_y(p):
            for d, to in enumerate(other_y):
                bulk.start(
                    remote(mine(p), slot(p, sp), bulk_y.at[p, 0, d], bulk_r.at[p, sp], to, tp)
                )

        middle = jnp.logical_and(z > 0, z < nz - 1)

        def source(up, d, also=None):
            src, cond = (sp - d * ny, z >= d) if up else (sp + d * ny, z < nz - d)
            return src, cond if also is None else jnp.logical_and(cond, also)

        def take(p, up, d, also=None):
            src, cond = source(up, d, also)
            src = jnp.clip(src, 0, n_sp - 1)
            arrived(slot(p, src), bulk_z.at[p, 0], bulk_r.at[p, src], cond)

        def on_z(p, up, d, also=None):
            src, cond = source(up, d, also)
            src = jnp.clip(src, 0, n_sp - 1)
            to, more = (sp + ny, z < nz - 1) if up else (sp - ny, z > 0)
            sem = bulk_z.at[p, 2 * d + (0 if up else 1)]
            bulk.start(
                remote(slot(p, src), slot(p, src), sem, bulk_r.at[p, src], to, tp),
                jnp.logical_and(cond, more),
            )

        balanced = ny == 2 and nz >= 4

        def by_y(p, src_z):
            if not balanced:
                return jnp.bool_(True)
            m, h = p // 2, p % 2
            skip = jnp.logical_or(
                jnp.logical_and(z == 1, src_z == 0),
                jnp.logical_and(z == nz - 2, src_z == nz - 1),
            )
            if m == 2 or h == 1:
                skip = jnp.logical_or(skip, jnp.logical_and(z == 0, src_z == 1))
            if h == 1:
                skip = jnp.logical_or(skip, jnp.logical_and(z == nz - 1, src_z == nz - 2))
            return jnp.logical_not(skip)

        def beside(p):
            m, h = p // 2, p % 2
            src = z * ny + (y + 1) % ny
            arrived(slot(p, src), bulk_z.at[p, 0], bulk_r.at[p, src])
            cond = jnp.logical_or(z == 0, z == nz - 1)
            if h == 1:
                cond = jnp.logical_or(cond, jnp.logical_or(z == 1, z == nz - 2))
            elif m == 2:
                cond = jnp.logical_or(cond, z == 1)
            down_to = jnp.logical_or(z == 1, z == nz - 1)
            to = jnp.where(down_to, z - 1, z + 1) * ny + y
            bulk.start(
                remote(slot(p, src), slot(p, src), bulk_z.at[p, 2 * nz], bulk_r.at[p, src], to, tp),
                cond,
            )

        def share(m):
            if balanced:
                beside(2 * m)
                beside(2 * m + 1)

        def on_y(p, up, d, also=None):
            src, cond = source(up, d, also)
            cond = jnp.logical_and(cond, by_y(p, src // ny))
            src = jnp.clip(src, 0, n_sp - 1)
            for e, to in enumerate(other_y):
                sem = bulk_y.at[p, 2 * d + (0 if up else 1), e]
                bulk.start(
                    remote(slot(p, src), slot(p, src), sem, bulk_r.at[p, src], to, tp), cond
                )

        def relay(m, up, d, also=None):
            if d >= nz:
                return
            for p in (2 * m, 2 * m + 1):
                take(p, up, d, also)
                if d < nz - 1:
                    on_z(p, up, d, also)
                on_y(p, up, d, also)

        def side_arrivals(m):
            for src in range(n_sp):
                for p in (2 * m, 2 * m + 1):
                    cond = src % ny != y
                    if balanced:
                        cond = jnp.logical_and(cond, src // ny != z)
                    arrived(slot(p, src), bulk_z.at[p, 0], bulk_r.at[p, src], cond)

        own_z(0, True)
        own_z(1, True, z > 0)
        for p in (0, 1, 2, 3):
            own_z(p, False)

        ii = lax.broadcasted_iota(jnp.int32, (BLOCK, BLOCK), 0)
        jj = lax.broadcasted_iota(jnp.int32, (BLOCK, BLOCK), 1)
        lower = (ii >= jj).astype(F32)
        logs = log_ref[...]
        cum_col[...] = dot_t(lower, logs, ((1,), (1,)), lax.Precision.HIGHEST)

        def column(idx):
            lane = lax.broadcasted_iota(jnp.int32, cum_col.shape, 1)
            return jnp.sum(jnp.where(lane == idx, cum_col[...], 0.0), axis=1, keepdims=True)

        def angles(b):
            row = pl.ds(sp * nb + b, 1)
            co, so = cos_out[row, :], sin_out[row, :]
            ci, si = cos_in[...], sin_in[...]
            return ci * co - si * so, si * co + ci * so

        def rotated(value, cosine, sine):
            front, second = value[:, :half_k], value[:, half_k:]
            return jnp.concatenate(
                [front * cosine - second * sine, front * sine + second * cosine], axis=1
            )

        def block_rows(b):
            return pl.ds(pl.multiple_of(b * BLOCK, BLOCK), BLOCK)

        loads[0].wait()
        loads[1].wait()
        st[...] = jnp.zeros_like(st)

        def local_states(b, _):
            r = block_rows(b)
            cosine, sine = angles(b)
            for h in range(heads):
                cc = column(h * nb + b)
                total = cc[BLOCK - 1 : BLOCK, :]
                kc = pl.ds(h * key_width, key_width)
                key = rotated(kb[r, kc].astype(F32), cosine, sine) * key_width ** (-0.5)
                key = key.astype(BF16)
                kb[r, kc] = key
                faded = (key.astype(F32) * jnp.exp(total - cc)).astype(BF16)
                term = dot_t(faded, vb[r, pl.ds(h * value_width, value_width)], ((0,), (0,)))
                before = st[h]
                lb[b * heads + h] = before.astype(BF16)
                st[h] = jnp.exp(total) * before + term
            return 0

        lax.fori_loop(0, nb, local_states, 0)

        def head_log(h):
            total = jnp.zeros((1, 1), F32)
            for b in range(nb):
                total = total + jnp.sum(logs[h * nb + b : h * nb + b + 1, :], axis=1, keepdims=True)
            return total

        hrow = lax.broadcasted_iota(jnp.int32, (8, 128), 0)
        tile = jnp.zeros((8, 128), F32)
        for h in range(heads):
            tile = jnp.where(hrow == h, head_log(h), tile)
        dec[pl.ds(y, 1)] = tile[None]
        states = Sends()
        for d, to in enumerate(other_y):
            far = (y + d + 1) % ny
            states.start(
                remote(dec.at[y], dec.at[y], dec_s.at[d], dec_r.at[y], to, tp)
            )
            for h in range(heads):
                for f in range(ny):

                    @pl.when(far == f)
                    def _():
                        xs[d, h] = st[h, :, f * slice_w : (f + 1) * slice_w].astype(BF16)

                states.start(
                    remote(xs.at[d, h], xr.at[y, h], st_s.at[d, h], st_r.at[y, h], to, tp)
                )
        own_y(0)
        own_y(1)

        loads[2].wait()

        def within_block(b, _):
            r = block_rows(b)
            cosine, sine = angles(b)
            for h in range(heads):
                cc = column(h * nb + b)
                kc = pl.ds(h * key_width, key_width)
                query = rotated(qb[r, kc].astype(F32), cosine, sine).astype(BF16)
                scores = dot_t(query, kb[r, kc], ((1,), (1,)))
                crow = jnp.sum(jnp.where(ii == jj, cc, 0.0), axis=0, keepdims=True)
                gap = jnp.where(ii >= jj, cc - crow, 0.0)
                weight = jnp.where(ii >= jj, jnp.exp(gap), 0.0)
                vc = pl.ds(h * value_width, value_width)
                within[r, vc] = dot((scores * weight).astype(BF16), vb[r, vc])
                qb[r, kc] = (query.astype(F32) * jnp.exp(cc)).astype(BF16)
            return 0

        lax.fori_loop(0, nb, within_block, 0)

        for f in range(ny):

            @pl.when(y == f)
            def _():
                for h in range(heads):
                    xr[f, h] = st[h, :, f * slice_w : (f + 1) * slice_w].astype(BF16)

        for d in range(1, ny):
            src = (y + d) % ny
            arrived(dec.at[src], dec_s.at[0], dec_r.at[src])
            for h in range(heads):
                arrived(xr.at[src, h], st_s.at[0, 0], st_r.at[src, h])
        for h in range(heads):

            @pl.when(z == 0)
            def _():
                chain_r[h] = jnp.zeros((key_width, slice_w), BF16)

            arrived(chain_r.at[h], ch_s.at[h], ch_r.at[h], z > 0)
            incoming = chain_r[h].astype(F32)
            before = incoming
            for f in range(ny):
                cb_mine = before.astype(BF16)

                @pl.when(y == f)
                def _():
                    cb[y, h] = cb_mine

                @pl.when(y != f)
                def _():
                    cs[f, h] = cb_mine

                decay = jnp.exp(dec[f, h : h + 1, 0:1])
                before = decay * before + xr[f, h].astype(F32)
            chain_s[h] = before.astype(BF16)
            states.start(
                remote(chain_s.at[h], chain_r.at[h], ch_s.at[h], ch_r.at[h], sp + ny, tp),
                z < nz - 1,
            )
            for d, to in enumerate(other_y):
                far = (y + d + 1) % ny
                states.start(
                    remote(cs.at[far, h], cb.at[y, h], cb_s.at[d, h], cb_r.at[y, h], to, tp)
                )

        own_z(1, True, z == 0)
        for p in (2, 3):
            own_z(p, True)
            own_y(p)
        relay(0, False, 1)
        share(0)

        loads[3].wait()
        for h in range(heads):
            for d in range(1, ny):
                src = (y + d) % ny
                arrived(cb.at[src, h], cb_s.at[0, 0], cb_r.at[src, h])

            def finish(b, decay):
                r = block_rows(b)
                vc = pl.ds(h * value_width, value_width)
                state = jnp.concatenate([cb[f, h].astype(F32) for f in range(ny)], axis=1)
                state = (decay * state + lb[b * heads + h].astype(F32)).astype(BF16)
                mixed = within[r, vc] + dot(qb[r, pl.ds(h * key_width, key_width)], state)
                average = jnp.mean(mixed, axis=1, keepdims=True)
                mixed = mixed - average
                spread = jnp.mean(mixed * mixed, axis=1, keepdims=True)
                gate = gb[r, vc].astype(F32)
                gated = gate * jax.nn.sigmoid(gate) * (mixed * lax.rsqrt(spread + tiny_stabilizer))
                gb[r, vc] = gated.astype(BF16)
                return decay * jnp.exp(column(h * nb + b)[BLOCK - 1 : BLOCK, :])

            lax.fori_loop(0, nb, finish, jnp.ones((1, 1), F32))
        states.drain()
        relay(0, True, 1)

        def owner_rows(xx, cc):
            return pl.ds(pl.multiple_of((xx * cores + cc) * own, own), own)

        def piece_cols(s):
            return pl.ds(pl.multiple_of(s * piece, piece), piece)

        def d2d_copies(s):
            return [
                remote(
                    part.at[s, owner_rows(xx, (c + d) % cores)], r1.at[s, d - 1, xx],
                    rs1_s.at[s, d - 1, xx], rs1_r.at[s, d - 1, xx],
                    sp, x * cores + (c + d) % cores,
                )
                for d in range(1, cores)
                for xx in range(lines)
            ]

        def x_copies(s):
            return [
                remote(
                    s2.at[s, d - 1], r2.at[s, d - 1], rs2_s.at[s, d - 1], rs2_r.at[s, d - 1],
                    sp, (x + d) % lines * cores + c,
                )
                for d in range(1, lines)
            ]

        row_tile = min(tok_rows, 512)

        def product(s, lhs, rhs):
            def one(i, _):
                r = pl.ds(pl.multiple_of(i * row_tile, row_tile), row_tile)
                part[s, r, :] = dot(lhs[r, :], rhs()).astype(BF16)
                return 0

            lax.fori_loop(0, tok_rows // row_tile, one, 0)
            for copy in d2d_copies(s):
                copy.start()

        def combine(s):
            for copy in d2d_copies(s):
                copy.wait_recv()
            for d in range(lines):
                xx = (x + d) % lines
                total = part[s, owner_rows(xx, c), :].astype(F32)
                for e in range(cores - 1):
                    total = total + r1[s, e, xx].astype(F32)
                if d == 0:
                    acc[:, piece_cols(s)] = total
                else:
                    s2[s, d - 1] = total.astype(BF16)
            for copy in x_copies(s):
                copy.start()

        def collect(s):
            for copy in x_copies(s):
                copy.wait_recv()
            total = acc[:, piece_cols(s)]
            for d in range(lines - 1):
                total = total + r2[s, d].astype(F32)
            acc[:, piece_cols(s)] = total

        def release(s, _):
            for copy in d2d_copies(s) + x_copies(s):
                copy.wait_send()
            return 0

        def out_step(s, _):
            product(s, gb, lambda: ow[:, piece_cols(s)])
            pl.when(s > 0)(lambda: combine(s - 1))
            return 0

        loads[4].wait()
        lax.fori_loop(0, n_sp, out_step, 0)
        combine(n_sp - 1)
        relay(0, False, 2)
        relay(0, True, 2)
        relay(1, False, 1)
        relay(1, True, 1)

        def collect_step(s, _):
            collect(s)
            return 0

        lax.fori_loop(0, n_sp, collect_step, 0)

        loads[5].wait()

        def layer_norm(values, which):
            average = jnp.mean(values, axis=1, keepdims=True)
            values = values - average
            spread = jnp.mean(values * values, axis=1, keepdims=True)
            values = values * lax.rsqrt(spread + tiny_stabilizer)
            return values * gain[which : which + 1, :] + bias[which : which + 1, :]

        ln_rows = 32
        gathered = Sends()

        def chunk_of(owner, j):
            return rows.at[pl.ds(pl.multiple_of(HALO + owner * own + j * chunk, 16), chunk)]

        pl.when(sp == 0)(lambda: rows.__setitem__((pl.ds(0, HALO), slice(None)), jnp.zeros((HALO, width), BF16)))
        for j in range(ROW_CHUNKS):

            def norm_rows(i, _):
                at = pl.multiple_of(j * chunk + i * ln_rows, ln_rows)
                r = pl.ds(at, ln_rows)
                value = layer_norm(alpha_scale * res[r, :].astype(F32) + acc[r, :], 0).astype(BF16)
                res[r, :] = value
                rows[pl.ds(pl.multiple_of(HALO + tp * own + at, 16), ln_rows), :] = value
                return 0

            lax.fori_loop(0, chunk // ln_rows, norm_rows, 0)
            for d, to in enumerate(other_c + other_x):
                gathered.start(
                    remote(chunk_of(tp, j), chunk_of(tp, j), ag_s.at[j, d], ag_r.at[j, tp], sp, to)
                )
        last = pl.ds(tok_rows, HALO)
        for t in range(n_tp):
            gathered.start(
                remote(rows.at[last], rows.at[pl.ds(0, HALO)], halo_s.at[t], halo_r, sp + 1, t),
                jnp.logical_and(tp == n_tp - 1, sp < n_sp - 1),
            )
        for j in range(ROW_CHUNKS):
            if j == ROW_CHUNKS // 2:
                relay(0, False, 3)
                relay(1, False, 2, z > 0)
                relay(1, True, 2, z < nz - 1)
                share(1)
            if j == ROW_CHUNKS - 1:
                relay(0, True, 3)
            for d in range(1, lines):
                owner = (x + d) % lines * cores + c
                arrived(chunk_of(owner, j), ag_s.at[j, 0], ag_r.at[j, owner])
                for e, to in enumerate(other_c):
                    gathered.start(
                        remote(
                            chunk_of(owner, j), chunk_of(owner, j),
                            agf_s.at[j, d - 1, e], ag_r.at[j, owner], sp, to,
                        )
                    )
        for d in range(1, cores):
            for e in range(lines):
                owner = (x + e) % lines * cores + (c + d) % cores
                for j in range(ROW_CHUNKS):
                    arrived(chunk_of(owner, j), ag_s.at[j, 0], ag_r.at[j, owner])
        for p in (4, 5):
            own_z(p, False)
            own_z(p, True)
        relay(1, False, 2, z == 0)
        relay(1, True, 2, z == nz - 1)
        for d in range(4, nz):
            relay(0, False, d)
            relay(0, True, d)
        lax.fori_loop(0, n_sp, release, 0)

        def up_tile(m, start, count):
            r = pl.ds(start, count)
            total = None
            for s in range(n_sp):
                term = dot(rows[r, s * depth : (s + 1) * depth], wg[s, m])
                total = term if total is None else total + term
            ups[m, r, :] = total.astype(BF16)

        def up_rows(m):
            def one(i, _):
                up_tile(m, pl.multiple_of(HALO + i * BLOCK, 16), BLOCK)
                return 0

            lax.fori_loop(0, tok_rows // BLOCK, one, 0)
            up_tile(m, 0, HALO)

        loads[6].wait()
        side_arrivals(0)
        arrived(rows.at[pl.ds(0, HALO)], halo_s.at[0], halo_r, sp > 0)
        up_rows(0)
        for d in range(3, nz):
            relay(1, False, d)
            relay(1, True, d)
        own_y(4)
        own_y(5)
        relay(2, False, 1, middle)
        relay(2, True, 1, middle)
        loads[7].wait()
        side_arrivals(1)
        up_rows(1)

        def activate(i, col):
            at = pl.multiple_of(i * BLOCK, BLOCK)
            convs = []
            for m in range(2):
                tile = ups[m, pl.ds(at, BLOCK + HALO), col].astype(F32)
                value = shift[m : m + 1, col]
                for j in range(3):
                    value = value + taps[m, j : j + 1, col] * tile[HALO - 2 + j : HALO - 2 + j + BLOCK, :]
                convs.append(value)
            act[pl.ds(at, BLOCK), col] = (jax.nn.gelu(convs[0]) * convs[1]).astype(BF16)

        def activate_step(i, _):
            for t in range(hidden // hcols):
                activate(i, pl.ds(t * hcols, hcols))
            return 0

        lax.fori_loop(0, tok_rows // BLOCK, activate_step, 0)

        order = [
            [zz] + sorted((o for o in range(nz) if o != zz), key=lambda o: (abs(o - zz), abs(2 * o - nz + 1)))
            for zz in range(nz)
        ]

        def nearest(k):
            got = jnp.int32(order[0][k])
            for zz in range(1, nz):
                got = jnp.where(z == zz, order[zz][k], got)
            return got

        first = [(k, 0) for k in range(nz)]
        second = [(k, d) for k in range(nz) for d in range(1, ny)]
        steps = first[:-1] + second[: ny - 1] + first[-1:] + second[ny - 1 :]
        loads[8].wait()
        previous = None
        done = []
        for k, d in steps:
            src_z = nearest(k)
            src = src_z * ny + (y + d) % ny
            if balanced and d > 0 and k == 0:
                share(2)
            elif d > 0:
                for p in (4, 5):
                    arrived(slot(p, src), bulk_z.at[p, 0], bulk_r.at[p, src])
            elif k > 0:
                to_z = jnp.where(src_z < z, z + 1, z - 1)
                more = jnp.logical_and(to_z >= 0, to_z < nz)
                fresh = jnp.logical_not(jnp.logical_and(middle, jnp.abs(src_z - z) == 1))
                for p in (4, 5):
                    arrived(slot(p, src), bulk_z.at[p, 0], bulk_r.at[p, src], fresh)
                    bulk.start(
                        remote(
                            slot(p, src), slot(p, src), bulk_z.at[p, 2 * nz + k],
                            bulk_r.at[p, src], to_z * ny + y, tp,
                        ),
                        jnp.logical_and(more, fresh),
                    )
                    for e, to in enumerate(other_y):
                        bulk.start(
                            remote(
                                slot(p, src), slot(p, src), bulk_y.at[p, 2 * nz + k, e],
                                bulk_r.at[p, src], to, tp,
                            ),
                            jnp.logical_and(by_y(p, src_z), fresh),
                        )
            product(src, act, lambda: wd[src])
            if previous is not None:
                combine(previous)
            previous = src
            done.append(src)
        combine(previous)
        for src in done:
            collect(src)

        def final_rows(i, _):
            r = pl.ds(pl.multiple_of(i * ln_rows, ln_rows), ln_rows)
            out[r, :] = layer_norm(alpha_scale * res[r, :].astype(F32) + acc[r, :], 1).astype(BF16)
            return 0

        lax.fori_loop(0, own // ln_rows, final_rows, 0)
        lax.fori_loop(0, n_sp, release, 0)
        gathered.drain()
        bulk.drain()

    vmem, dma = pltpu.VMEM, pltpu.SemaphoreType.DMA
    oc, ol, oy = max(cores - 1, 1), max(lines - 1, 1), max(ny - 1, 1)
    scratch = [
        vmem((n_sp, 2, depth, hidden), BF16),
        vmem((n_sp, hidden, piece), BF16),
        vmem((tok_rows, heads * key_width), BF16),
        vmem((tok_rows, heads * key_width), BF16),
        vmem((tok_rows, heads * value_width), BF16),
        vmem((tok_rows, heads * value_width), BF16),
        vmem((heads * value_width, width), BF16),
        vmem((own, width), BF16),
        vmem((BLOCK, heads * nb), F32),
        vmem((heads, key_width, value_width), F32),
        vmem((nb * heads, key_width, value_width), BF16),
        vmem((tok_rows, heads * value_width), F32),
        vmem((oy, heads, key_width, slice_w), BF16),
        vmem((ny, heads, key_width, slice_w), BF16),
        vmem((ny, 8, 128), F32),
        vmem((heads, key_width, slice_w), BF16),
        vmem((heads, key_width, slice_w), BF16),
        vmem((ny, heads, key_width, slice_w), BF16),
        vmem((ny, heads, key_width, slice_w), BF16),
        vmem((n_sp, tok_rows, piece), BF16),
        vmem((n_sp, oc, lines, own, piece), BF16),
        vmem((n_sp, ol, own, piece), BF16),
        vmem((n_sp, ol, own, piece), BF16),
        vmem((own, width), F32),
        vmem((HALO + tok_rows, width), BF16),
        vmem((2, HALO + tok_rows, hidden), BF16),
        vmem((tok_rows, hidden), BF16),
        dma((9,)),
        dma((6, n_sp)),
        dma((6, 3 * nz)),
        dma((6, 3 * nz, oy)),
        dma((oy, heads)),
        dma((ny, heads)),
        dma((oy,)),
        dma((ny,)),
        dma((heads,)),
        dma((heads,)),
        dma((oy, heads)),
        dma((ny, heads)),
        dma((n_sp, oc, lines)),
        dma((n_sp, oc, lines)),
        dma((n_sp, ol)),
        dma((n_sp, ol)),
        dma((ROW_CHUNKS, cores + lines)),
        dma((ROW_CHUNKS, n_tp)),
        dma((ROW_CHUNKS, ol, oc)),
        dma((n_tp,)),
        dma(()),
    ]
    in_specs = [pl.BlockSpec(memory_space=pltpu.VMEM)] * 9 + [pl.BlockSpec(memory_space=pl.ANY)] * 9
    return pl.pallas_call(
        kernel,
        out_shape=jax.ShapeDtypeStruct((own, width), BF16),
        in_specs=in_specs,
        out_specs=pl.BlockSpec(memory_space=pltpu.VMEM),
        scratch_shapes=scratch,
        compiler_params=pltpu.CompilerParams(
            collective_id=0, has_side_effects=True, vmem_limit_bytes=67_000_000
        ),
    )


def make_square_kernel(n_sp, n_tp, tok_rows, heads, key_width, value_width, width, depth, hidden):
    cores, lines, ny, nz = layout(n_sp, n_tp)
    nb = tok_rows // BLOCK
    own = tok_rows // n_tp
    piece = width // n_sp
    slice_w = value_width // ny
    half_k = key_width // 2
    dh, hh = depth // 2, hidden // 2
    chunk = own // ROW_CHUNKS
    hcols = 128 if hidden % 128 == 0 else hidden

    def kernel(
        cos_in, sin_in, cos_out, sin_out, log_ref, gain, bias, taps, shift,
        q_hbm, k_hbm, v_hbm, g_hbm, res_hbm, ow_hbm, upg, upv, down,
        out,
        tapb, shiftb, wg, wd, qb, kb, vb, gb, ow, res, cum_col, st, lb, within,
        xs, xr, dec, chain_s, chain_r, cb, cs, part, r1, s2, r2, acc, rows, ups, act,
        load_sem, bulk_r, bulk_z, bulk_y, bulk_c, tap_s, tap_r, st_s, st_r, dec_s, dec_r, ch_s, ch_r, cb_s, cb_r,
        rs1_s, rs1_r, rs2_s, rs2_r, ag_s, ag_r, halo_s, halo_r, f1_s, f1_r, f2_s, f2_r,
    ):
        sp, tp = lax.axis_index("sp"), lax.axis_index("tp")
        z, y = sp // ny, sp % ny
        x, c = tp // cores, tp % cores
        me = z * ny + c
        straight = c == y
        crossed = jnp.logical_not(straight)
        cross_sp, cross_tp = z * ny + c, x * cores + y
        by_c = x * cores + 1 - c
        by_x = (1 - x) * cores + c
        by_y = z * ny + 1 - y

        def remote(src, dst, ssem, rsem, to_sp, to_tp):
            return pltpu.make_async_remote_copy(
                src_ref=src, dst_ref=dst, send_sem=ssem, recv_sem=rsem,
                device_id=(to_sp, to_tp), device_id_type=MESH,
            )

        def arrived(dst, ssem, rsem, cond=None):
            copy = remote(dst, dst, ssem, rsem, sp, tp)
            if cond is None:
                copy.wait_recv()
            else:
                pl.when(cond)(copy.wait_recv)

        own_rows = pl.ds(pl.multiple_of(tp * own, own), own)
        pairs = [
            (k_hbm, kb), (v_hbm, vb), (q_hbm, qb), (g_hbm, gb), (ow_hbm, ow), (res_hbm.at[own_rows], res),
        ]
        loads = [pltpu.make_async_copy(a, b, load_sem.at[i]) for i, (a, b) in enumerate(pairs)]
        for load in loads:
            load.start()
        pairs = [(upg, wg.at[me, 0]), (upv, wg.at[me, 1]), (down, wd.at[me])]
        weight_loads = [
            pltpu.make_async_copy(a, b, load_sem.at[6 + i]) for i, (a, b) in enumerate(pairs)
        ]
        for load in weight_loads:
            pl.when(straight)(load.start)

        barrier = pltpu.get_barrier_semaphore()

        def greet(to_sp, to_tp, cond=None):
            def go():
                pl.semaphore_signal(barrier, inc=1, device_id=(to_sp, to_tp), device_id_type=MESH)

            if cond is None:
                go()
            else:
                pl.when(cond)(go)

        other_y = [z * ny + (y + d) % ny for d in range(1, ny)]
        last_x = jnp.logical_and(c == 1, x == lines - 1)
        next_sp = jnp.where(last_x, sp + 1, sp)
        next_x = jnp.where(c == 0, x, jnp.where(last_x, 0, x + 1))
        has_next = jnp.logical_or(jnp.logical_not(last_x), sp < n_sp - 1)
        next_z = next_sp // ny
        next_seg = next_sp % ny * lines + next_x
        halo_to = [
            (next_z * ny + yy, xx * cores + 1 - c, has_next) for yy in range(ny) for xx in range(lines)
        ]
        halo_from = []
        for yy in range(ny):
            for xx in range(lines):
                here = z * ny + yy
                if xx > 0:
                    halo_from.append((here, jnp.where(c == 1, xx * cores, (xx - 1) * cores + 1), None))
                else:
                    halo_from.append(
                        (
                            jnp.where(c == 1, here, here - 1),
                            jnp.where(c == 1, 0, (lines - 1) * cores + 1),
                            jnp.logical_or(c == 1, here > 0),
                        )
                    )
        other_c = [x * cores + (c + d) % cores for d in range(1, cores)]
        other_x = [(x + d) % lines * cores + c for d in range(1, lines)]
        peers = [(sp + ny, tp, z < nz - 1), (sp - ny, tp, z > 0)]
        peers += [(o, tp, None) for o in other_y]
        peers += [(sp, o, None) for o in other_c + other_x]
        peers += [(cross_sp, cross_tp, crossed)]
        peers += halo_to + halo_from
        for to_sp, to_tp, cond in peers:
            greet(to_sp, to_tp, cond)
        count = jnp.int32(0)
        for _, _, cond in peers:
            count = count + (1 if cond is None else cond.astype(jnp.int32))
        pl.semaphore_wait(barrier, count)

        bulk = Sends()

        def slot(p, src):
            m, h = p // 2, p % 2
            if m < 2:
                return wg.at[src, m, pl.ds(h * dh, dh)]
            return wd.at[src, pl.ds(h * hh, hh)]

        def mine(p):
            m, h = p // 2, p % 2
            if m == 2:
                return down.at[pl.ds(h * hh, hh)]
            return (upg, upv)[m].at[pl.ds(h * dh, dh)]

        def cross(p):
            bulk.start(
                remote(mine(p), slot(p, sp), bulk_y.at[p], bulk_r.at[p, sp], cross_sp, cross_tp), crossed
            )

        def own_z(p, up, also=None):
            cond, to = (z < nz - 1, sp + ny) if up else (z > 0, sp - ny)
            cond = jnp.logical_and(cond, straight)
            if also is not None:
                cond = jnp.logical_and(cond, also)
            bulk.start(
                remote(mine(p), slot(p, me), bulk_z.at[p, 0 if up else 1], bulk_r.at[p, me], to, tp),
                cond,
            )

        def own_c(p):
            bulk.start(
                remote(mine(p), slot(p, me), bulk_c.at[p, 0], bulk_r.at[p, me], sp, by_c), straight
            )

        def crossed_own(p):
            arrived(slot(p, me), bulk_y.at[p], bulk_r.at[p, me], crossed)
            for up in (False, True):
                cond, to = (z < nz - 1, sp + ny) if up else (z > 0, sp - ny)
                bulk.start(
                    remote(
                        slot(p, me), slot(p, me), bulk_z.at[p, 2 if up else 3], bulk_r.at[p, me], to, tp
                    ),
                    jnp.logical_and(cond, crossed),
                )
            bulk.start(
                remote(slot(p, me), slot(p, me), bulk_c.at[p, 1], bulk_r.at[p, me], sp, by_c), crossed
            )

        middle = jnp.logical_and(z > 0, z < nz - 1)

        def source(up, d, also=None):
            src, cond = (me - d * ny, z >= d) if up else (me + d * ny, z < nz - d)
            return src, cond if also is None else jnp.logical_and(cond, also)

        def take(p, up, d, also=None):
            src, cond = source(up, d, also)
            src = jnp.clip(src, 0, n_sp - 1)
            arrived(slot(p, src), bulk_z.at[p, 0], bulk_r.at[p, src], cond)

        def on_z(p, up, d, also=None):
            src, cond = source(up, d, also)
            src = jnp.clip(src, 0, n_sp - 1)
            to, more = (sp + ny, z < nz - 1) if up else (sp - ny, z > 0)
            sem = bulk_z.at[p, 2 + 2 * d + (0 if up else 1)]
            bulk.start(
                remote(slot(p, src), slot(p, src), sem, bulk_r.at[p, src], to, tp),
                jnp.logical_and(cond, more),
            )

        def on_c(p, up, d, also=None):
            src, cond = source(up, d, also)
            src = jnp.clip(src, 0, n_sp - 1)
            sem = bulk_c.at[p, 2 * d + (0 if up else 1)]
            bulk.start(
                remote(slot(p, src), slot(p, src), sem, bulk_r.at[p, src], sp, by_c), cond
            )

        def relay(m, up, d, also=None):
            if d >= nz:
                return
            for p in (2 * m, 2 * m + 1):
                take(p, up, d, also)
                if d < nz - 1:
                    on_z(p, up, d, also)
                on_c(p, up, d, also)

        def side_arrivals(m):
            for zz in range(nz):
                for p in (2 * m, 2 * m + 1):
                    src = zz * ny + 1 - c
                    arrived(slot(p, src), bulk_z.at[p, 0], bulk_r.at[p, src])

        own_z(0, True)
        own_z(1, True, z > 0)
        for p in (0, 1, 2, 3):
            own_z(p, False)

        ii = lax.broadcasted_iota(jnp.int32, (BLOCK, BLOCK), 0)
        jj = lax.broadcasted_iota(jnp.int32, (BLOCK, BLOCK), 1)
        lower = (ii >= jj).astype(F32)
        logs = log_ref[...]
        cum_col[...] = dot_t(lower, logs, ((1,), (1,)), lax.Precision.HIGHEST)

        def column(idx):
            lane = lax.broadcasted_iota(jnp.int32, cum_col.shape, 1)
            return jnp.sum(jnp.where(lane == idx, cum_col[...], 0.0), axis=1, keepdims=True)

        def angles(b):
            row = pl.ds(sp * nb + b, 1)
            co, so = cos_out[row, :], sin_out[row, :]
            ci, si = cos_in[...], sin_in[...]
            return ci * co - si * so, si * co + ci * so

        def rotated(value, cosine, sine):
            front, second = value[:, :half_k], value[:, half_k:]
            return jnp.concatenate(
                [front * cosine - second * sine, front * sine + second * cosine], axis=1
            )

        def block_rows(b):
            return pl.ds(pl.multiple_of(b * BLOCK, BLOCK), BLOCK)

        loads[0].wait()
        loads[1].wait()
        st[...] = jnp.zeros_like(st)

        def local_states(b, _):
            r = block_rows(b)
            cosine, sine = angles(b)
            for h in range(heads):
                cc = column(h * nb + b)
                total = cc[BLOCK - 1 : BLOCK, :]
                kc = pl.ds(h * key_width, key_width)
                key = rotated(kb[r, kc].astype(F32), cosine, sine) * key_width ** (-0.5)
                key = key.astype(BF16)
                kb[r, kc] = key
                faded = (key.astype(F32) * jnp.exp(total - cc)).astype(BF16)
                term = dot_t(faded, vb[r, pl.ds(h * value_width, value_width)], ((0,), (0,)))
                before = st[h]
                lb[b * heads + h] = before.astype(BF16)
                st[h] = jnp.exp(total) * before + term
            return 0

        lax.fori_loop(0, nb, local_states, 0)

        def head_log(h):
            total = jnp.zeros((1, 1), F32)
            for b in range(nb):
                total = total + jnp.sum(logs[h * nb + b : h * nb + b + 1, :], axis=1, keepdims=True)
            return total

        hrow = lax.broadcasted_iota(jnp.int32, (8, 128), 0)
        tile = jnp.zeros((8, 128), F32)
        for h in range(heads):
            tile = jnp.where(hrow == h, head_log(h), tile)
        dec[pl.ds(y, 1)] = tile[None]
        states = Sends()
        for d, to in enumerate(other_y):
            far = (y + d + 1) % ny
            states.start(
                remote(dec.at[y], dec.at[y], dec_s.at[d], dec_r.at[y], to, tp)
            )
            for h in range(heads):
                for f in range(ny):

                    @pl.when(far == f)
                    def _():
                        xs[d, h] = st[h, :, f * slice_w : (f + 1) * slice_w].astype(BF16)

                states.start(
                    remote(xs.at[d, h], xr.at[y, h], st_s.at[d, h], st_r.at[y, h], to, tp)
                )
        cross(0)
        cross(1)

        loads[2].wait()

        def within_block(b, _):
            r = block_rows(b)
            cosine, sine = angles(b)
            for h in range(heads):
                cc = column(h * nb + b)
                kc = pl.ds(h * key_width, key_width)
                query = rotated(qb[r, kc].astype(F32), cosine, sine).astype(BF16)
                scores = dot_t(query, kb[r, kc], ((1,), (1,)))
                crow = jnp.sum(jnp.where(ii == jj, cc, 0.0), axis=0, keepdims=True)
                gap = jnp.where(ii >= jj, cc - crow, 0.0)
                weight = jnp.where(ii >= jj, jnp.exp(gap), 0.0)
                vc = pl.ds(h * value_width, value_width)
                within[r, vc] = dot((scores * weight).astype(BF16), vb[r, vc])
                qb[r, kc] = (query.astype(F32) * jnp.exp(cc)).astype(BF16)
            return 0

        lax.fori_loop(0, nb, within_block, 0)

        for f in range(ny):

            @pl.when(y == f)
            def _():
                for h in range(heads):
                    xr[f, h] = st[h, :, f * slice_w : (f + 1) * slice_w].astype(BF16)

        for d in range(1, ny):
            src = (y + d) % ny
            arrived(dec.at[src], dec_s.at[0], dec_r.at[src])
            for h in range(heads):
                arrived(xr.at[src, h], st_s.at[0, 0], st_r.at[src, h])
        for h in range(heads):

            @pl.when(z == 0)
            def _():
                chain_r[h] = jnp.zeros((key_width, slice_w), BF16)

            arrived(chain_r.at[h], ch_s.at[h], ch_r.at[h], z > 0)
            incoming = chain_r[h].astype(F32)
            before = incoming
            for f in range(ny):
                cb_mine = before.astype(BF16)

                @pl.when(y == f)
                def _():
                    cb[y, h] = cb_mine

                @pl.when(y != f)
                def _():
                    cs[f, h] = cb_mine

                decay = jnp.exp(dec[f, h : h + 1, 0:1])
                before = decay * before + xr[f, h].astype(F32)
            chain_s[h] = before.astype(BF16)
            states.start(
                remote(chain_s.at[h], chain_r.at[h], ch_s.at[h], ch_r.at[h], sp + ny, tp),
                z < nz - 1,
            )
            for d, to in enumerate(other_y):
                far = (y + d + 1) % ny
                states.start(
                    remote(cs.at[far, h], cb.at[y, h], cb_s.at[d, h], cb_r.at[y, h], to, tp)
                )

        own_z(1, True, z == 0)
        for p in (2, 3):
            own_z(p, True)
        for p in range(4):
            own_c(p)
        for p in (2, 3, 4, 5):
            cross(p)
        bulk.start(remote(taps, tapb, tap_s.at[0], tap_r.at[0], cross_sp, cross_tp), crossed)
        bulk.start(remote(shift, shiftb, tap_s.at[1], tap_r.at[1], cross_sp, cross_tp), crossed)

        @pl.when(straight)
        def _():
            tapb[...] = taps[...]
            shiftb[...] = shift[...]

        crossed_own(0)
        crossed_own(1)
        relay(0, False, 1, straight)

        loads[3].wait()
        for h in range(heads):
            for d in range(1, ny):
                src = (y + d) % ny
                arrived(cb.at[src, h], cb_s.at[0, 0], cb_r.at[src, h])

            def finish(b, decay):
                r = block_rows(b)
                vc = pl.ds(h * value_width, value_width)
                state = jnp.concatenate([cb[f, h].astype(F32) for f in range(ny)], axis=1)
                state = (decay * state + lb[b * heads + h].astype(F32)).astype(BF16)
                mixed = within[r, vc] + dot(qb[r, pl.ds(h * key_width, key_width)], state)
                average = jnp.mean(mixed, axis=1, keepdims=True)
                mixed = mixed - average
                spread = jnp.mean(mixed * mixed, axis=1, keepdims=True)
                gate = gb[r, vc].astype(F32)
                gated = gate * jax.nn.sigmoid(gate) * (mixed * lax.rsqrt(spread + tiny_stabilizer))
                gb[r, vc] = gated.astype(BF16)
                return decay * jnp.exp(column(h * nb + b)[BLOCK - 1 : BLOCK, :])

            lax.fori_loop(0, nb, finish, jnp.ones((1, 1), F32))
        states.drain()

        def owner_rows(xx, cc):
            return pl.ds(pl.multiple_of((xx * cores + cc) * own, own), own)

        def piece_cols(s):
            return pl.ds(pl.multiple_of(s * piece, piece), piece)

        def d2d_copies(s):
            return [
                remote(
                    part.at[s, owner_rows(xx, (c + d) % cores)], r1.at[s, d - 1, xx],
                    rs1_s.at[s, d - 1, xx], rs1_r.at[s, d - 1, xx],
                    sp, x * cores + (c + d) % cores,
                )
                for d in range(1, cores)
                for xx in range(lines)
            ]

        def x_copies(s):
            return [
                remote(
                    s2.at[s, d - 1], r2.at[s, d - 1], rs2_s.at[s, d - 1], rs2_r.at[s, d - 1],
                    sp, (x + d) % lines * cores + c,
                )
                for d in range(1, lines)
            ]

        row_tile = min(tok_rows, 512)

        def product(s, lhs, rhs):
            def one(i, _):
                r = pl.ds(pl.multiple_of(i * row_tile, row_tile), row_tile)
                part[s, r, :] = dot(lhs[r, :], rhs()).astype(BF16)
                return 0

            lax.fori_loop(0, tok_rows // row_tile, one, 0)
            for copy in d2d_copies(s):
                copy.start()

        def combine(s):
            for copy in d2d_copies(s):
                copy.wait_recv()
            for d in range(lines):
                xx = (x + d) % lines
                total = part[s, owner_rows(xx, c), :].astype(F32)
                for e in range(cores - 1):
                    total = total + r1[s, e, xx].astype(F32)
                if d == 0:
                    acc[:, piece_cols(s)] = total
                else:
                    s2[s, d - 1] = total.astype(BF16)
            for copy in x_copies(s):
                copy.start()

        def collect(s):
            for copy in x_copies(s):
                copy.wait_recv()
            total = acc[:, piece_cols(s)]
            for d in range(lines - 1):
                total = total + r2[s, d].astype(F32)
            acc[:, piece_cols(s)] = total

        def release(s, _):
            for copy in d2d_copies(s) + x_copies(s):
                copy.wait_send()
            return 0

        def out_step(s, _):
            product(s, gb, lambda: ow[:, piece_cols(s)])
            pl.when(s > 0)(lambda: combine(s - 1))
            return 0

        loads[4].wait()
        lax.fori_loop(0, n_sp, out_step, 0)
        combine(n_sp - 1)
        crossed_own(2)
        crossed_own(3)
        relay(0, False, 1, crossed)
        relay(0, True, 1)
        relay(0, False, 2)
        relay(0, True, 2)
        relay(1, False, 1)
        relay(1, True, 1)

        def collect_step(s, _):
            collect(s)
            return 0

        lax.fori_loop(0, n_sp, collect_step, 0)

        loads[5].wait()

        def layer_norm(values, which):
            average = jnp.mean(values, axis=1, keepdims=True)
            values = values - average
            spread = jnp.mean(values * values, axis=1, keepdims=True)
            values = values * lax.rsqrt(spread + tiny_stabilizer)
            return values * gain[which : which + 1, :] + bias[which : which + 1, :]

        ln_rows = 32
        gathered = Sends()

        seg = HALO + own

        def chunk_of(yy, xx, j):
            at = (yy * lines + xx) * seg + HALO + j * chunk
            return rows.at[pl.ds(pl.multiple_of(at, 16), chunk)]

        def gather_sem(j, yy, xx):
            return ag_r.at[j, yy * lines + xx]

        for yy in range(ny):
            for xx in range(lines):
                if yy == 0 and xx == 0:

                    @pl.when(jnp.logical_and(z == 0, c == 0))
                    def _():
                        rows[pl.ds(0, HALO), :] = jnp.zeros((HALO, width), BF16)

        for j in range(ROW_CHUNKS):

            def norm_rows(i, _):
                at = pl.multiple_of(j * chunk + i * ln_rows, ln_rows)
                r = pl.ds(at, ln_rows)
                value = layer_norm(alpha_scale * res[r, :].astype(F32) + acc[r, :], 0).astype(BF16)
                res[r, :] = value
                rows[pl.ds(pl.multiple_of((y * lines + x) * seg + HALO + at, 16), ln_rows), :] = value
                return 0

            lax.fori_loop(0, chunk // ln_rows, norm_rows, 0)
            mine_now = chunk_of(y, x, j)
            gathered.start(remote(mine_now, mine_now, ag_s.at[j, 0], gather_sem(j, y, x), sp, by_x))
            gathered.start(remote(mine_now, mine_now, ag_s.at[j, 1], gather_sem(j, y, x), by_y, tp))
        tail = rows.at[pl.ds(pl.multiple_of((y * lines + x) * seg + own, 16), HALO)]
        head = rows.at[pl.ds(pl.multiple_of(next_seg * seg, 16), HALO)]
        for t, (to_sp, to_tp, cond) in enumerate(halo_to):
            gathered.start(remote(tail, head, halo_s.at[t], halo_r.at[next_seg], to_sp, to_tp), cond)
        for j in range(ROW_CHUNKS):
            if j == ROW_CHUNKS // 2:
                relay(0, False, 3)
                relay(1, False, 2, z > 0)
                relay(1, True, 2, z < nz - 1)
            if j == ROW_CHUNKS - 1:
                relay(0, True, 3)
            got = chunk_of(y, 1 - x, j)
            arrived(got, ag_s.at[j, 0], gather_sem(j, y, 1 - x))
            if j % 2 == 0:
                gathered.start(remote(got, got, ag_s.at[j, 2], gather_sem(j, y, 1 - x), by_y, tp))
            got = chunk_of(1 - y, x, j)
            arrived(got, ag_s.at[j, 0], gather_sem(j, 1 - y, x))
            if j % 2 == 1:
                gathered.start(remote(got, got, ag_s.at[j, 2], gather_sem(j, 1 - y, x), sp, by_x))
        for p in (4, 5):
            own_z(p, False)
            own_z(p, True)
            own_c(p)
            crossed_own(p)
        for j in range(ROW_CHUNKS):
            arrived(chunk_of(1 - y, 1 - x, j), ag_s.at[j, 0], gather_sem(j, 1 - y, 1 - x))
        relay(1, False, 2, z == 0)
        relay(1, True, 2, z == nz - 1)
        for d in range(4, nz):
            relay(0, False, d)
            relay(0, True, d)
        lax.fori_loop(0, n_sp, release, 0)

        def up_tile(m, start, count):
            r = pl.ds(start, count)
            total = None
            for s in range(n_sp):
                term = dot(rows[r, s * depth : (s + 1) * depth], wg[s, m])
                total = term if total is None else total + term
            ups[m, r, :] = total.astype(BF16)

        def up_rows(m):
            def one(i, _):
                up_tile(m, pl.multiple_of(i * seg, 16), seg)
                return 0

            lax.fori_loop(0, n_tp, one, 0)

        pl.when(straight)(weight_loads[0].wait)
        side_arrivals(0)
        for g, (_, _, cond) in enumerate(halo_from):
            arrived(rows.at[pl.ds(g * seg, HALO)], halo_s.at[0], halo_r.at[g], cond)
        up_rows(0)
        for d in range(3, nz):
            relay(1, False, d)
            relay(1, True, d)
        relay(2, False, 1, middle)
        relay(2, True, 1, middle)
        pl.when(straight)(weight_loads[1].wait)
        side_arrivals(1)
        up_rows(1)

        arrived(tapb, tap_s.at[0], tap_r.at[0], crossed)
        arrived(shiftb, tap_s.at[1], tap_r.at[1], crossed)

        def activate(i, col):
            at = pl.multiple_of(i * seg, 16)
            convs = []
            for m in range(2):
                tile = ups[m, pl.ds(at, seg), col].astype(F32)
                value = shiftb[m : m + 1, col]
                for j in range(3):
                    value = value + tapb[m, j : j + 1, col] * tile[HALO - 2 + j : HALO - 2 + j + own, :]
                convs.append(value)
            act[pl.ds(pl.multiple_of(i * own, 16), own), col] = (
                jax.nn.gelu(convs[0]) * convs[1]
            ).astype(BF16)

        def activate_step(i, _):
            for t in range(hidden // hcols):
                activate(i, pl.ds(t * hcols, hcols))
            return 0

        lax.fori_loop(0, n_tp, activate_step, 0)

        order = [
            [zz] + sorted((o for o in range(nz) if o != zz), key=lambda o: (abs(o - zz), abs(2 * o - nz + 1)))
            for zz in range(nz)
        ]

        def nearest(k):
            got = jnp.int32(order[0][k])
            for zz in range(1, nz):
                got = jnp.where(z == zz, order[zz][k], got)
            return got

        half = piece // 2
        left, right = pl.ds(0, half), pl.ds(half, half)

        def seg_rows(yy, xx):
            return pl.ds(pl.multiple_of((yy * lines + xx) * own, own), own)

        def first_hops(s):
            copies = [
                remote(
                    part.at[s, seg_rows(yy, 1 - x), left], r1.at[s, 0, yy, :, left],
                    f1_s.at[s, yy], f1_r.at[s, yy], sp, by_x,
                )
                for yy in range(ny)
            ]
            return copies + [
                remote(
                    part.at[s, seg_rows(1 - y, xx), right], r1.at[s, 0, xx, :, right],
                    f1_s.at[s, ny + xx], f1_r.at[s, ny + xx], by_y, tp,
                )
                for xx in range(lines)
            ]

        def second_hops(s):
            return [
                remote(
                    s2.at[s, 0, :, left], r2.at[s, 0, :, left], f2_s.at[s, 0], f2_r.at[s, 0], by_y, tp
                ),
                remote(
                    s2.at[s, 0, :, right], r2.at[s, 0, :, right], f2_s.at[s, 1], f2_r.at[s, 1], sp, by_x
                ),
            ]

        def halves(s):
            at = pl.multiple_of(s * piece, piece)
            return pl.ds(at, half), pl.ds(pl.multiple_of(at + half, half), half)

        def down_step(s):
            def one(i, _):
                r = pl.ds(pl.multiple_of(i * row_tile, row_tile), row_tile)
                part[s, r, :] = dot(act[r, :], wd[s]).astype(BF16)
                return 0

            lax.fori_loop(0, tok_rows // row_tile, one, 0)
            for copy in first_hops(s):
                copy.start()

        def down_combine(s):
            for copy in first_hops(s):
                copy.wait_recv()
            lcols, rcols = halves(s)

            def summed(yy, xx, other, cols):
                return part[s, seg_rows(yy, xx), cols].astype(F32) + r1[s, 0, other, :, cols].astype(F32)

            s2[s, 0, :, left] = summed(1 - y, x, 1 - y, left).astype(BF16)
            s2[s, 0, :, right] = summed(y, 1 - x, 1 - x, right).astype(BF16)
            for copy in second_hops(s):
                copy.start()
            acc[:, lcols] = summed(y, x, y, left)
            acc[:, rcols] = summed(y, x, x, right)

        def down_collect(s):
            for copy in second_hops(s):
                copy.wait_recv()
            acc[:, piece_cols(s)] = acc[:, piece_cols(s)] + r2[s, 0].astype(F32)

        def down_release(s, _):
            for copy in first_hops(s) + second_hops(s):
                copy.wait_send()
            return 0

        pl.when(straight)(weight_loads[2].wait)
        previous = None
        done = []
        for k in range(nz):
            src_z = nearest(k)
            if k > 0:
                src = src_z * ny + c
                to_z = jnp.where(src_z < z, z + 1, z - 1)
                more = jnp.logical_and(to_z >= 0, to_z < nz)
                fresh = jnp.logical_not(jnp.logical_and(middle, jnp.abs(src_z - z) == 1))
                for p in (4, 5):
                    arrived(slot(p, src), bulk_z.at[p, 0], bulk_r.at[p, src], fresh)
                    bulk.start(
                        remote(
                            slot(p, src), slot(p, src), bulk_z.at[p, 2 * nz + 2 + k],
                            bulk_r.at[p, src], to_z * ny + y, tp,
                        ),
                        jnp.logical_and(more, fresh),
                    )
                    bulk.start(
                        remote(
                            slot(p, src), slot(p, src), bulk_c.at[p, 2 * nz + k],
                            bulk_r.at[p, src], sp, by_c,
                        ),
                        fresh,
                    )
            for d in range(cores):
                src = src_z * ny + (c + d) % cores
                if d > 0:
                    for p in (4, 5):
                        arrived(slot(p, src), bulk_z.at[p, 0], bulk_r.at[p, src])
                down_step(src)
                if previous is not None:
                    down_combine(previous)
                previous = src
                done.append(src)
        down_combine(previous)
        for src in done:
            down_collect(src)

        def final_rows(i, _):
            r = pl.ds(pl.multiple_of(i * ln_rows, ln_rows), ln_rows)
            out[r, :] = layer_norm(alpha_scale * res[r, :].astype(F32) + acc[r, :], 1).astype(BF16)
            return 0

        lax.fori_loop(0, own // ln_rows, final_rows, 0)
        lax.fori_loop(0, n_sp, down_release, 0)
        gathered.drain()
        bulk.drain()

    vmem, dma = pltpu.VMEM, pltpu.SemaphoreType.DMA
    oc, ol, oy = max(cores - 1, 1), max(lines - 1, 1), max(ny - 1, 1)
    scratch = [
        vmem((2, 3, hidden), F32),
        vmem((2, hidden), F32),
        vmem((n_sp, 2, depth, hidden), BF16),
        vmem((n_sp, hidden, piece), BF16),
        vmem((tok_rows, heads * key_width), BF16),
        vmem((tok_rows, heads * key_width), BF16),
        vmem((tok_rows, heads * value_width), BF16),
        vmem((tok_rows, heads * value_width), BF16),
        vmem((heads * value_width, width), BF16),
        vmem((own, width), BF16),
        vmem((BLOCK, heads * nb), F32),
        vmem((heads, key_width, value_width), F32),
        vmem((nb * heads, key_width, value_width), BF16),
        vmem((tok_rows, heads * value_width), F32),
        vmem((oy, heads, key_width, slice_w), BF16),
        vmem((ny, heads, key_width, slice_w), BF16),
        vmem((ny, 8, 128), F32),
        vmem((heads, key_width, slice_w), BF16),
        vmem((heads, key_width, slice_w), BF16),
        vmem((ny, heads, key_width, slice_w), BF16),
        vmem((ny, heads, key_width, slice_w), BF16),
        vmem((n_sp, tok_rows, piece), BF16),
        vmem((n_sp, oc, lines, own, piece), BF16),
        vmem((n_sp, ol, own, piece), BF16),
        vmem((n_sp, ol, own, piece), BF16),
        vmem((own, width), F32),
        vmem((n_tp * HALO + tok_rows, width), BF16),
        vmem((2, n_tp * HALO + tok_rows, hidden), BF16),
        vmem((tok_rows, hidden), BF16),
        dma((9,)),
        dma((6, n_sp)),
        dma((6, 3 * nz + 2)),
        dma((6,)),
        dma((6, 3 * nz)),
        dma((2,)),
        dma((2,)),
        dma((oy, heads)),
        dma((ny, heads)),
        dma((oy,)),
        dma((ny,)),
        dma((heads,)),
        dma((heads,)),
        dma((oy, heads)),
        dma((ny, heads)),
        dma((n_sp, oc, lines)),
        dma((n_sp, oc, lines)),
        dma((n_sp, ol)),
        dma((n_sp, ol)),
        dma((ROW_CHUNKS, 3)),
        dma((ROW_CHUNKS, n_tp)),
        dma((n_tp,)),
        dma((n_tp,)),
        dma((n_sp, ny + lines)),
        dma((n_sp, ny + lines)),
        dma((n_sp, 2)),
        dma((n_sp, 2)),
    ]
    in_specs = [pl.BlockSpec(memory_space=pltpu.VMEM)] * 9 + [pl.BlockSpec(memory_space=pl.ANY)] * 9
    return pl.pallas_call(
        kernel,
        out_shape=jax.ShapeDtypeStruct((own, width), BF16),
        in_specs=in_specs,
        out_specs=pl.BlockSpec(memory_space=pltpu.VMEM),
        scratch_shapes=scratch,
        compiler_params=pltpu.CompilerParams(
            collective_id=0, has_side_effects=True, vmem_limit_bytes=67_000_000
        ),
    )


def shards(
    query_proj, key_proj, value_proj, gate_proj, log_decay, residual, out_weight, norm_gain,
    norm_bias, up_gate, up_value, conv_weight, conv_bias, down_weight,
):
    n_sp, n_tp = lax.axis_size("sp"), lax.axis_size("tp")
    tok_rows, heads = log_decay.shape
    key_width = query_proj.shape[1] // heads
    value_width = value_proj.shape[1] // heads
    nb = tok_rows // BLOCK
    cores, lines, ny, _ = layout(n_sp, n_tp)
    make = make_square_kernel if cores == lines == ny == 2 else make_kernel
    call = make(
        n_sp, n_tp, tok_rows, heads, key_width, value_width,
        residual.shape[1], up_gate.shape[0], up_gate.shape[1],
    )
    tables = rotary_tables(key_width, n_sp * nb)
    logs = log_decay.T.reshape(heads * nb, BLOCK)
    return call(
        *tables, logs, norm_gain, norm_bias, conv_weight, conv_bias, query_proj, key_proj,
        value_proj, gate_proj, residual, out_weight, up_gate, up_value, down_weight,
    )


def solution(mesh):
    placed = (
        P("sp", "tp"), P("sp", "tp"), P("sp", "tp"), P("sp", "tp"), P("sp", "tp"),
        P("sp", None), P("tp", None), P(), P(), P("sp", "tp"), P("sp", "tp"),
        P(None, None, "tp"), P(None, "tp"), P("tp", "sp"),
    )
    return jax.shard_map(
        shards, mesh=mesh, in_specs=placed, out_specs=P(("sp", "tp"), None), check_vma=False
    )
```

```python
import numpy as np
import jax
import jax.numpy as jnp
from jax import lax
from jax.experimental import pallas as pl
from jax.experimental.pallas import tpu as pltpu
from jax.sharding import PartitionSpec as P

BLOCK = 256
HALO = 16
ROW_CHUNKS = 4

alpha_scale = 8.0**0.25
rope_base = 10000.0
tiny_stabilizer = 1e-05
MESH = pl.DeviceIdType.MESH
F32, BF16 = jnp.float32, jnp.bfloat16


def dot(a, b):
    return jnp.dot(a, b, preferred_element_type=F32)


def dot_t(a, b, dims, precision=None):
    return lax.dot_general(a, b, (dims, ((), ())), precision=precision, preferred_element_type=F32)


def layout(sp, tp):
    cores = 2 if tp % 2 == 0 else 1
    lines = tp // cores
    ny = lines if sp % lines == 0 else 1
    return cores, lines, ny, sp // ny


def rotary_tables(head_width, blocks):
    half = head_width // 2
    freq = rope_base ** (-2.0 * np.arange(half, dtype=np.float64) / head_width)
    inner = np.arange(BLOCK, dtype=np.float64)[:, None] * freq
    outer = (np.arange(blocks, dtype=np.float64) * BLOCK)[:, None] * freq
    tables = (np.cos(inner), np.sin(inner), np.cos(outer), np.sin(outer))
    return [jnp.asarray(t.astype(np.float32)) for t in tables]


class Sends:
    def __init__(self):
        self.left = []

    def start(self, copy, cond=None):
        self.left.append((copy, cond))
        if cond is None:
            copy.start()
        else:
            pl.when(cond)(copy.start)

    def drain(self):
        for copy, cond in self.left:
            if cond is None:
                copy.wait_send()
            else:
                pl.when(cond)(copy.wait_send)
        self.left = []


def make_kernel(n_sp, n_tp, tok_rows, heads, key_width, value_width, width, depth, hidden):
    cores, lines, ny, nz = layout(n_sp, n_tp)
    nb = tok_rows // BLOCK
    own = tok_rows // n_tp
    piece = width // n_sp
    slice_w = value_width // ny
    half_k = key_width // 2
    dh, hh = depth // 2, hidden // 2
    chunk = own // ROW_CHUNKS
    hcols = 128 if hidden % 128 == 0 else hidden

    def kernel(
        cos_in, sin_in, cos_out, sin_out, log_ref, gain, bias, taps, shift,
        q_hbm, k_hbm, v_hbm, g_hbm, res_hbm, ow_hbm, upg, upv, down,
        out,
        wg, wd, qb, kb, vb, gb, ow, res, cum_col, st, lb, within,
        xs, xr, dec, chain_s, chain_r, cb, cs, part, r1, s2, r2, acc, rows, ups, act,
        load_sem, bulk_r, bulk_z, bulk_y, st_s, st_r, dec_s, dec_r, ch_s, ch_r, cb_s, cb_r,
        rs1_s, rs1_r, rs2_s, rs2_r, ag_s, ag_r, agf_s, halo_s, halo_r,
    ):
        sp, tp = lax.axis_index("sp"), lax.axis_index("tp")
        z, y = sp // ny, sp % ny
        x, c = tp // cores, tp % cores
        me_sp = sp

        def remote(src, dst, ssem, rsem, to_sp, to_tp):
            return pltpu.make_async_remote_copy(
                src_ref=src, dst_ref=dst, send_sem=ssem, recv_sem=rsem,
                device_id=(to_sp, to_tp), device_id_type=MESH,
            )

        def arrived(dst, ssem, rsem, cond=None):
            copy = remote(dst, dst, ssem, rsem, sp, tp)
            if cond is None:
                copy.wait_recv()
            else:
                pl.when(cond)(copy.wait_recv)

        own_rows = pl.ds(pl.multiple_of(tp * own, own), own)
        pairs = [
            (k_hbm, kb), (v_hbm, vb), (q_hbm, qb), (g_hbm, gb), (ow_hbm, ow),
            (res_hbm.at[own_rows], res), (upg, wg.at[me_sp, 0]), (upv, wg.at[me_sp, 1]),
            (down, wd.at[me_sp]),
        ]
        loads = [pltpu.make_async_copy(a, b, load_sem.at[i]) for i, (a, b) in enumerate(pairs)]
        for load in loads:
            load.start()

        barrier = pltpu.get_barrier_semaphore()

        def greet(to_sp, to_tp, cond=None):
            def go():
                pl.semaphore_signal(barrier, inc=1, device_id=(to_sp, to_tp), device_id_type=MESH)

            if cond is None:
                go()
            else:
                pl.when(cond)(go)

        other_y = [z * ny + (y + d) % ny for d in range(1, ny)]
        other_c = [x * cores + (c + d) % cores for d in range(1, cores)]
        other_x = [(x + d) % lines * cores + c for d in range(1, lines)]
        peers = [(sp + ny, tp, z < nz - 1), (sp - ny, tp, z > 0)]
        peers += [(o, tp, None) for o in other_y]
        peers += [(sp, o, None) for o in other_c + other_x]
        for t in range(n_tp):
            peers.append((sp + 1, t, jnp.logical_and(tp == n_tp - 1, sp < n_sp - 1)))
        for to_sp, to_tp, cond in peers:
            greet(to_sp, to_tp, cond)
        greet(sp - 1, n_tp - 1, sp > 0)
        count = (sp > 0).astype(jnp.int32)
        for _, _, cond in peers:
            count = count + (1 if cond is None else cond.astype(jnp.int32))
        pl.semaphore_wait(barrier, count)

        bulk = Sends()

        def slot(p, src):
            m, h = p // 2, p % 2
            if m < 2:
                return wg.at[src, m, pl.ds(h * dh, dh)]
            return wd.at[src, pl.ds(h * hh, hh)]

        def mine(p):
            m, h = p // 2, p % 2
            if m == 2:
                return down.at[pl.ds(h * hh, hh)]
            return (upg, upv)[m].at[pl.ds(h * dh, dh)]

        def own_z(p, up, also=None):
            cond, to = (z < nz - 1, sp + ny) if up else (z > 0, sp - ny)
            if also is not None:
                cond = jnp.logical_and(cond, also)
            bulk.start(
                remote(mine(p), slot(p, sp), bulk_z.at[p, 0 if up else 1], bulk_r.at[p, sp], to, tp),
                cond,
            )

        def own_y(p):
            for d, to in enumerate(other_y):
                bulk.start(
                    remote(mine(p), slot(p, sp), bulk_y.at[p, 0, d], bulk_r.at[p, sp], to, tp)
                )

        middle = jnp.logical_and(z > 0, z < nz - 1)

        def source(up, d, also=None):
            src, cond = (sp - d * ny, z >= d) if up else (sp + d * ny, z < nz - d)
            return src, cond if also is None else jnp.logical_and(cond, also)

        def take(p, up, d, also=None):
            src, cond = source(up, d, also)
            src = jnp.clip(src, 0, n_sp - 1)
            arrived(slot(p, src), bulk_z.at[p, 0], bulk_r.at[p, src], cond)

        def on_z(p, up, d, also=None):
            src, cond = source(up, d, also)
            src = jnp.clip(src, 0, n_sp - 1)
            to, more = (sp + ny, z < nz - 1) if up else (sp - ny, z > 0)
            sem = bulk_z.at[p, 2 * d + (0 if up else 1)]
            bulk.start(
                remote(slot(p, src), slot(p, src), sem, bulk_r.at[p, src], to, tp),
                jnp.logical_and(cond, more),
            )

        balanced = ny == 2 and nz >= 4

        def by_y(p, src_z):
            if not balanced:
                return jnp.bool_(True)
            m, h = p // 2, p % 2
            skip = jnp.logical_or(
                jnp.logical_and(z == 1, src_z == 0),
                jnp.logical_and(z == nz - 2, src_z == nz - 1),
            )
            if m == 2 or h == 1:
                skip = jnp.logical_or(skip, jnp.logical_and(z == 0, src_z == 1))
            if h == 1:
                skip = jnp.logical_or(skip, jnp.logical_and(z == nz - 1, src_z == nz - 2))
            return jnp.logical_not(skip)

        def beside(p):
            m, h = p // 2, p % 2
            src = z * ny + (y + 1) % ny
            arrived(slot(p, src), bulk_z.at[p, 0], bulk_r.at[p, src])
            cond = jnp.logical_or(z == 0, z == nz - 1)
            if h == 1:
                cond = jnp.logical_or(cond, jnp.logical_or(z == 1, z == nz - 2))
            elif m == 2:
                cond = jnp.logical_or(cond, z == 1)
            down_to = jnp.logical_or(z == 1, z == nz - 1)
            to = jnp.where(down_to, z - 1, z + 1) * ny + y
            bulk.start(
                remote(slot(p, src), slot(p, src), bulk_z.at[p, 2 * nz], bulk_r.at[p, src], to, tp),
                cond,
            )

        def share(m):
            if balanced:
                beside(2 * m)
                beside(2 * m + 1)

        def on_y(p, up, d, also=None):
            src, cond = source(up, d, also)
            cond = jnp.logical_and(cond, by_y(p, src // ny))
            src = jnp.clip(src, 0, n_sp - 1)
            for e, to in enumerate(other_y):
                sem = bulk_y.at[p, 2 * d + (0 if up else 1), e]
                bulk.start(
                    remote(slot(p, src), slot(p, src), sem, bulk_r.at[p, src], to, tp), cond
                )

        def relay(m, up, d, also=None):
            if d >= nz:
                return
            for p in (2 * m, 2 * m + 1):
                take(p, up, d, also)
                if d < nz - 1:
                    on_z(p, up, d, also)
                on_y(p, up, d, also)

        def side_arrivals(m):
            for src in range(n_sp):
                for p in (2 * m, 2 * m + 1):
                    cond = src % ny != y
                    if balanced:
                        cond = jnp.logical_and(cond, src // ny != z)
                    arrived(slot(p, src), bulk_z.at[p, 0], bulk_r.at[p, src], cond)

        own_z(0, True)
        own_z(1, True, z > 0)
        for p in (0, 1, 2, 3):
            own_z(p, False)

        ii = lax.broadcasted_iota(jnp.int32, (BLOCK, BLOCK), 0)
        jj = lax.broadcasted_iota(jnp.int32, (BLOCK, BLOCK), 1)
        lower = (ii >= jj).astype(F32)
        logs = log_ref[...]
        cum_col[...] = dot_t(lower, logs, ((1,), (1,)), lax.Precision.HIGHEST)

        def column(idx):
            lane = lax.broadcasted_iota(jnp.int32, cum_col.shape, 1)
            return jnp.sum(jnp.where(lane == idx, cum_col[...], 0.0), axis=1, keepdims=True)

        def angles(b):
            row = pl.ds(sp * nb + b, 1)
            co, so = cos_out[row, :], sin_out[row, :]
            ci, si = cos_in[...], sin_in[...]
            return ci * co - si * so, si * co + ci * so

        def rotated(value, cosine, sine):
            front, second = value[:, :half_k], value[:, half_k:]
            return jnp.concatenate(
                [front * cosine - second * sine, front * sine + second * cosine], axis=1
            )

        def block_rows(b):
            return pl.ds(pl.multiple_of(b * BLOCK, BLOCK), BLOCK)

        loads[0].wait()
        loads[1].wait()
        st[...] = jnp.zeros_like(st)

        def local_states(b, _):
            r = block_rows(b)
            cosine, sine = angles(b)
            for h in range(heads):
                cc = column(h * nb + b)
                total = cc[BLOCK - 1 : BLOCK, :]
                kc = pl.ds(h * key_width, key_width)
                key = rotated(kb[r, kc].astype(F32), cosine, sine) * key_width ** (-0.5)
                key = key.astype(BF16)
                kb[r, kc] = key
                faded = (key.astype(F32) * jnp.exp(total - cc)).astype(BF16)
                term = dot_t(faded, vb[r, pl.ds(h * value_width, value_width)], ((0,), (0,)))
                before = st[h]
                lb[b * heads + h] = before.astype(BF16)
                st[h] = jnp.exp(total) * before + term
            return 0

        lax.fori_loop(0, nb, local_states, 0)

        def head_log(h):
            total = jnp.zeros((1, 1), F32)
            for b in range(nb):
                total = total + jnp.sum(logs[h * nb + b : h * nb + b + 1, :], axis=1, keepdims=True)
            return total

        hrow = lax.broadcasted_iota(jnp.int32, (8, 128), 0)
        tile = jnp.zeros((8, 128), F32)
        for h in range(heads):
            tile = jnp.where(hrow == h, head_log(h), tile)
        dec[pl.ds(y, 1)] = tile[None]
        states = Sends()
        for d, to in enumerate(other_y):
            far = (y + d + 1) % ny
            states.start(
                remote(dec.at[y], dec.at[y], dec_s.at[d], dec_r.at[y], to, tp)
            )
            for h in range(heads):
                for f in range(ny):

                    @pl.when(far == f)
                    def _():
                        xs[d, h] = st[h, :, f * slice_w : (f + 1) * slice_w].astype(BF16)

                states.start(
                    remote(xs.at[d, h], xr.at[y, h], st_s.at[d, h], st_r.at[y, h], to, tp)
                )
        own_y(0)
        own_y(1)

        loads[2].wait()

        def within_block(b, _):
            r = block_rows(b)
            cosine, sine = angles(b)
            for h in range(heads):
                cc = column(h * nb + b)
                kc = pl.ds(h * key_width, key_width)
                query = rotated(qb[r, kc].astype(F32), cosine, sine).astype(BF16)
                scores = dot_t(query, kb[r, kc], ((1,), (1,)))
                crow = jnp.sum(jnp.where(ii == jj, cc, 0.0), axis=0, keepdims=True)
                gap = jnp.where(ii >= jj, cc - crow, 0.0)
                weight = jnp.where(ii >= jj, jnp.exp(gap), 0.0)
                vc = pl.ds(h * value_width, value_width)
                within[r, vc] = dot((scores * weight).astype(BF16), vb[r, vc])
                qb[r, kc] = (query.astype(F32) * jnp.exp(cc)).astype(BF16)
            return 0

        lax.fori_loop(0, nb, within_block, 0)

        for f in range(ny):

            @pl.when(y == f)
            def _():
                for h in range(heads):
                    xr[f, h] = st[h, :, f * slice_w : (f + 1) * slice_w].astype(BF16)

        for d in range(1, ny):
            src = (y + d) % ny
            arrived(dec.at[src], dec_s.at[0], dec_r.at[src])
            for h in range(heads):
                arrived(xr.at[src, h], st_s.at[0, 0], st_r.at[src, h])
        for h in range(heads):

            @pl.when(z == 0)
            def _():
                chain_r[h] = jnp.zeros((key_width, slice_w), BF16)

            arrived(chain_r.at[h], ch_s.at[h], ch_r.at[h], z > 0)
            incoming = chain_r[h].astype(F32)
            before = incoming
            for f in range(ny):
                cb_mine = before.astype(BF16)

                @pl.when(y == f)
                def _():
                    cb[y, h] = cb_mine

                @pl.when(y != f)
                def _():
                    cs[f, h] = cb_mine

                decay = jnp.exp(dec[f, h : h + 1, 0:1])
                before = decay * before + xr[f, h].astype(F32)
            chain_s[h] = before.astype(BF16)
            states.start(
                remote(chain_s.at[h], chain_r.at[h], ch_s.at[h], ch_r.at[h], sp + ny, tp),
                z < nz - 1,
            )
            for d, to in enumerate(other_y):
                far = (y + d + 1) % ny
                states.start(
                    remote(cs.at[far, h], cb.at[y, h], cb_s.at[d, h], cb_r.at[y, h], to, tp)
                )

        own_z(1, True, z == 0)
        for p in (2, 3):
            own_z(p, True)
            own_y(p)
        relay(0, False, 1)
        share(0)

        loads[3].wait()
        for h in range(heads):
            for d in range(1, ny):
                src = (y + d) % ny
                arrived(cb.at[src, h], cb_s.at[0, 0], cb_r.at[src, h])

            def finish(b, decay):
                r = block_rows(b)
                vc = pl.ds(h * value_width, value_width)
                state = jnp.concatenate([cb[f, h].astype(F32) for f in range(ny)], axis=1)
                state = (decay * state + lb[b * heads + h].astype(F32)).astype(BF16)
                mixed = within[r, vc] + dot(qb[r, pl.ds(h * key_width, key_width)], state)
                average = jnp.mean(mixed, axis=1, keepdims=True)
                mixed = mixed - average
                spread = jnp.mean(mixed * mixed, axis=1, keepdims=True)
                gate = gb[r, vc].astype(F32)
                gated = gate * jax.nn.sigmoid(gate) * (mixed * lax.rsqrt(spread + tiny_stabilizer))
                gb[r, vc] = gated.astype(BF16)
                return decay * jnp.exp(column(h * nb + b)[BLOCK - 1 : BLOCK, :])

            lax.fori_loop(0, nb, finish, jnp.ones((1, 1), F32))
        states.drain()
        relay(0, True, 1)

        def owner_rows(xx, cc):
            return pl.ds(pl.multiple_of((xx * cores + cc) * own, own), own)

        def piece_cols(s):
            return pl.ds(pl.multiple_of(s * piece, piece), piece)

        def d2d_copies(s):
            return [
                remote(
                    part.at[s, owner_rows(xx, (c + d) % cores)], r1.at[s, d - 1, xx],
                    rs1_s.at[s, d - 1, xx], rs1_r.at[s, d - 1, xx],
                    sp, x * cores + (c + d) % cores,
                )
                for d in range(1, cores)
                for xx in range(lines)
            ]

        def x_copies(s):
            return [
                remote(
                    s2.at[s, d - 1], r2.at[s, d - 1], rs2_s.at[s, d - 1], rs2_r.at[s, d - 1],
                    sp, (x + d) % lines * cores + c,
                )
                for d in range(1, lines)
            ]

        row_tile = min(tok_rows, 512)

        def product(s, lhs, rhs):
            def one(i, _):
                r = pl.ds(pl.multiple_of(i * row_tile, row_tile), row_tile)
                part[s, r, :] = dot(lhs[r, :], rhs()).astype(BF16)
                return 0

            lax.fori_loop(0, tok_rows // row_tile, one, 0)
            for copy in d2d_copies(s):
                copy.start()

        def combine(s):
            for copy in d2d_copies(s):
                copy.wait_recv()
            for d in range(lines):
                xx = (x + d) % lines
                total = part[s, owner_rows(xx, c), :].astype(F32)
                for e in range(cores - 1):
                    total = total + r1[s, e, xx].astype(F32)
                if d == 0:
                    acc[:, piece_cols(s)] = total
                else:
                    s2[s, d - 1] = total.astype(BF16)
            for copy in x_copies(s):
                copy.start()

        def collect(s):
            for copy in x_copies(s):
                copy.wait_recv()
            total = acc[:, piece_cols(s)]
            for d in range(lines - 1):
                total = total + r2[s, d].astype(F32)
            acc[:, piece_cols(s)] = total

        def release(s, _):
            for copy in d2d_copies(s) + x_copies(s):
                copy.wait_send()
            return 0

        def out_step(s, _):
            product(s, gb, lambda: ow[:, piece_cols(s)])
            pl.when(s > 0)(lambda: combine(s - 1))
            return 0

        loads[4].wait()
        lax.fori_loop(0, n_sp, out_step, 0)
        combine(n_sp - 1)
        relay(0, False, 2)
        relay(0, True, 2)
        relay(1, False, 1)
        relay(1, True, 1)

        def collect_step(s, _):
            collect(s)
            return 0

        lax.fori_loop(0, n_sp, collect_step, 0)

        loads[5].wait()

        def layer_norm(values, which):
            average = jnp.mean(values, axis=1, keepdims=True)
            values = values - average
            spread = jnp.mean(values * values, axis=1, keepdims=True)
            values = values * lax.rsqrt(spread + tiny_stabilizer)
            return values * gain[which : which + 1, :] + bias[which : which + 1, :]

        ln_rows = 32
        gathered = Sends()

        def chunk_of(owner, j):
            return rows.at[pl.ds(pl.multiple_of(HALO + owner * own + j * chunk, 16), chunk)]

        pl.when(sp == 0)(lambda: rows.__setitem__((pl.ds(0, HALO), slice(None)), jnp.zeros((HALO, width), BF16)))
        for j in range(ROW_CHUNKS):

            def norm_rows(i, _):
                at = pl.multiple_of(j * chunk + i * ln_rows, ln_rows)
                r = pl.ds(at, ln_rows)
                value = layer_norm(alpha_scale * res[r, :].astype(F32) + acc[r, :], 0).astype(BF16)
                res[r, :] = value
                rows[pl.ds(pl.multiple_of(HALO + tp * own + at, 16), ln_rows), :] = value
                return 0

            lax.fori_loop(0, chunk // ln_rows, norm_rows, 0)
            for d, to in enumerate(other_c + other_x):
                gathered.start(
                    remote(chunk_of(tp, j), chunk_of(tp, j), ag_s.at[j, d], ag_r.at[j, tp], sp, to)
                )
        last = pl.ds(tok_rows, HALO)
        for t in range(n_tp):
            gathered.start(
                remote(rows.at[last], rows.at[pl.ds(0, HALO)], halo_s.at[t], halo_r, sp + 1, t),
                jnp.logical_and(tp == n_tp - 1, sp < n_sp - 1),
            )
        for j in range(ROW_CHUNKS):
            if j == ROW_CHUNKS // 2:
                relay(0, False, 3)
                relay(1, False, 2, z > 0)
                relay(1, True, 2, z < nz - 1)
                share(1)
            if j == ROW_CHUNKS - 1:
                relay(0, True, 3)
            for d in range(1, lines):
                owner = (x + d) % lines * cores + c
                arrived(chunk_of(owner, j), ag_s.at[j, 0], ag_r.at[j, owner])
                for e, to in enumerate(other_c):
                    gathered.start(
                        remote(
                            chunk_of(owner, j), chunk_of(owner, j),
                            agf_s.at[j, d - 1, e], ag_r.at[j, owner], sp, to,
                        )
                    )
        for d in range(1, cores):
            for e in range(lines):
                owner = (x + e) % lines * cores + (c + d) % cores
                for j in range(ROW_CHUNKS):
                    arrived(chunk_of(owner, j), ag_s.at[j, 0], ag_r.at[j, owner])
        for p in (4, 5):
            own_z(p, False)
            own_z(p, True)
        relay(1, False, 2, z == 0)
        relay(1, True, 2, z == nz - 1)
        for d in range(4, nz):
            relay(0, False, d)
            relay(0, True, d)
        lax.fori_loop(0, n_sp, release, 0)

        def up_tile(m, start, count):
            r = pl.ds(start, count)
            total = None
            for s in range(n_sp):
                term = dot(rows[r, s * depth : (s + 1) * depth], wg[s, m])
                total = term if total is None else total + term
            ups[m, r, :] = total.astype(BF16)

        def up_rows(m):
            def one(i, _):
                up_tile(m, pl.multiple_of(HALO + i * BLOCK, 16), BLOCK)
                return 0

            lax.fori_loop(0, tok_rows // BLOCK, one, 0)
            up_tile(m, 0, HALO)

        loads[6].wait()
        side_arrivals(0)
        arrived(rows.at[pl.ds(0, HALO)], halo_s.at[0], halo_r, sp > 0)
        up_rows(0)
        for d in range(3, nz):
            relay(1, False, d)
            relay(1, True, d)
        own_y(4)
        own_y(5)
        relay(2, False, 1, middle)
        relay(2, True, 1, middle)
        loads[7].wait()
        side_arrivals(1)
        up_rows(1)

        def activate(i, col):
            at = pl.multiple_of(i * BLOCK, BLOCK)
            convs = []
            for m in range(2):
                tile = ups[m, pl.ds(at, BLOCK + HALO), col].astype(F32)
                value = shift[m : m + 1, col]
                for j in range(3):
                    value = value + taps[m, j : j + 1, col] * tile[HALO - 2 + j : HALO - 2 + j + BLOCK, :]
                convs.append(value)
            act[pl.ds(at, BLOCK), col] = (jax.nn.gelu(convs[0]) * convs[1]).astype(BF16)

        def activate_step(i, _):
            for t in range(hidden // hcols):
                activate(i, pl.ds(t * hcols, hcols))
            return 0

        lax.fori_loop(0, tok_rows // BLOCK, activate_step, 0)

        order = [
            [zz] + sorted((o for o in range(nz) if o != zz), key=lambda o: (abs(o - zz), abs(2 * o - nz + 1)))
            for zz in range(nz)
        ]

        def nearest(k):
            got = jnp.int32(order[0][k])
            for zz in range(1, nz):
                got = jnp.where(z == zz, order[zz][k], got)
            return got

        first = [(k, 0) for k in range(nz)]
        second = [(k, d) for k in range(nz) for d in range(1, ny)]
        steps = first[:-1] + second[: ny - 1] + first[-1:] + second[ny - 1 :]
        loads[8].wait()
        previous = None
        done = []
        for k, d in steps:
            src_z = nearest(k)
            src = src_z * ny + (y + d) % ny
            if balanced and d > 0 and k == 0:
                share(2)
            elif d > 0:
                for p in (4, 5):
                    arrived(slot(p, src), bulk_z.at[p, 0], bulk_r.at[p, src])
            elif k > 0:
                to_z = jnp.where(src_z < z, z + 1, z - 1)
                more = jnp.logical_and(to_z >= 0, to_z < nz)
                fresh = jnp.logical_not(jnp.logical_and(middle, jnp.abs(src_z - z) == 1))
                for p in (4, 5):
                    arrived(slot(p, src), bulk_z.at[p, 0], bulk_r.at[p, src], fresh)
                    bulk.start(
                        remote(
                            slot(p, src), slot(p, src), bulk_z.at[p, 2 * nz + k],
                            bulk_r.at[p, src], to_z * ny + y, tp,
                        ),
                        jnp.logical_and(more, fresh),
                    )
                    for e, to in enumerate(other_y):
                        bulk.start(
                            remote(
                                slot(p, src), slot(p, src), bulk_y.at[p, 2 * nz + k, e],
                                bulk_r.at[p, src], to, tp,
                            ),
                            jnp.logical_and(by_y(p, src_z), fresh),
                        )
            product(src, act, lambda: wd[src])
            if previous is not None:
                combine(previous)
            previous = src
            done.append(src)
        combine(previous)
        for src in done:
            collect(src)

        def final_rows(i, _):
            r = pl.ds(pl.multiple_of(i * ln_rows, ln_rows), ln_rows)
            out[r, :] = layer_norm(alpha_scale * res[r, :].astype(F32) + acc[r, :], 1).astype(BF16)
            return 0

        lax.fori_loop(0, own // ln_rows, final_rows, 0)
        lax.fori_loop(0, n_sp, release, 0)
        gathered.drain()
        bulk.drain()

    vmem, dma = pltpu.VMEM, pltpu.SemaphoreType.DMA
    oc, ol, oy = max(cores - 1, 1), max(lines - 1, 1), max(ny - 1, 1)
    scratch = [
        vmem((n_sp, 2, depth, hidden), BF16),
        vmem((n_sp, hidden, piece), BF16),
        vmem((tok_rows, heads * key_width), BF16),
        vmem((tok_rows, heads * key_width), BF16),
        vmem((tok_rows, heads * value_width), BF16),
        vmem((tok_rows, heads * value_width), BF16),
        vmem((heads * value_width, width), BF16),
        vmem((own, width), BF16),
        vmem((BLOCK, heads * nb), F32),
        vmem((heads, key_width, value_width), F32),
        vmem((nb * heads, key_width, value_width), BF16),
        vmem((tok_rows, heads * value_width), F32),
        vmem((oy, heads, key_width, slice_w), BF16),
        vmem((ny, heads, key_width, slice_w), BF16),
        vmem((ny, 8, 128), F32),
        vmem((heads, key_width, slice_w), BF16),
        vmem((heads, key_width, slice_w), BF16),
        vmem((ny, heads, key_width, slice_w), BF16),
        vmem((ny, heads, key_width, slice_w), BF16),
        vmem((n_sp, tok_rows, piece), BF16),
        vmem((n_sp, oc, lines, own, piece), BF16),
        vmem((n_sp, ol, own, piece), BF16),
        vmem((n_sp, ol, own, piece), BF16),
        vmem((own, width), F32),
        vmem((HALO + tok_rows, width), BF16),
        vmem((2, HALO + tok_rows, hidden), BF16),
        vmem((tok_rows, hidden), BF16),
        dma((9,)),
        dma((6, n_sp)),
        dma((6, 3 * nz)),
        dma((6, 3 * nz, oy)),
        dma((oy, heads)),
        dma((ny, heads)),
        dma((oy,)),
        dma((ny,)),
        dma((heads,)),
        dma((heads,)),
        dma((oy, heads)),
        dma((ny, heads)),
        dma((n_sp, oc, lines)),
        dma((n_sp, oc, lines)),
        dma((n_sp, ol)),
        dma((n_sp, ol)),
        dma((ROW_CHUNKS, cores + lines)),
        dma((ROW_CHUNKS, n_tp)),
        dma((ROW_CHUNKS, ol, oc)),
        dma((n_tp,)),
        dma(()),
    ]
    in_specs = [pl.BlockSpec(memory_space=pltpu.VMEM)] * 9 + [pl.BlockSpec(memory_space=pl.ANY)] * 9
    return pl.pallas_call(
        kernel,
        out_shape=jax.ShapeDtypeStruct((own, width), BF16),
        in_specs=in_specs,
        out_specs=pl.BlockSpec(memory_space=pltpu.VMEM),
        scratch_shapes=scratch,
        compiler_params=pltpu.CompilerParams(
            collective_id=0, has_side_effects=True, vmem_limit_bytes=67_000_000
        ),
    )


def make_square_kernel(n_sp, n_tp, tok_rows, heads, key_width, value_width, width, depth, hidden):
    cores, lines, ny, nz = layout(n_sp, n_tp)
    nb = tok_rows // BLOCK
    own = tok_rows // n_tp
    piece = width // n_sp
    slice_w = value_width // ny
    half_k = key_width // 2
    dh, hh = depth // 2, hidden // 2
    chunk = own // ROW_CHUNKS
    hcols = 128 if hidden % 128 == 0 else hidden

    def kernel(
        cos_in, sin_in, cos_out, sin_out, log_ref, gain, bias, taps, shift,
        q_hbm, k_hbm, v_hbm, g_hbm, res_hbm, ow_hbm, upg, upv, down,
        out,
        tapb, shiftb, wg, wd, qb, kb, vb, gb, ow, res, cum_col, st, lb, within,
        xs, xr, dec, chain_s, chain_r, cb, cs, part, r1, s2, r2, acc, rows, ups, act,
        load_sem, bulk_r, bulk_z, bulk_y, bulk_c, tap_s, tap_r, st_s, st_r, dec_s, dec_r, ch_s, ch_r, cb_s, cb_r,
        ag_s, ag_r, halo_s, halo_r, f1_s, f1_r, f2_s, f2_r,
    ):
        sp, tp = lax.axis_index("sp"), lax.axis_index("tp")
        z, y = sp // ny, sp % ny
        x, c = tp // cores, tp % cores
        me = z * ny + c
        straight = c == y
        crossed = jnp.logical_not(straight)
        cross_sp, cross_tp = z * ny + c, x * cores + y
        by_c = x * cores + 1 - c
        by_x = (1 - x) * cores + c
        by_y = z * ny + 1 - y

        def remote(src, dst, ssem, rsem, to_sp, to_tp):
            return pltpu.make_async_remote_copy(
                src_ref=src, dst_ref=dst, send_sem=ssem, recv_sem=rsem,
                device_id=(to_sp, to_tp), device_id_type=MESH,
            )

        def arrived(dst, ssem, rsem, cond=None):
            copy = remote(dst, dst, ssem, rsem, sp, tp)
            if cond is None:
                copy.wait_recv()
            else:
                pl.when(cond)(copy.wait_recv)

        own_rows = pl.ds(pl.multiple_of(tp * own, own), own)
        pairs = [
            (k_hbm, kb), (v_hbm, vb), (q_hbm, qb), (g_hbm, gb), (ow_hbm, ow), (res_hbm.at[own_rows], res),
        ]
        loads = [pltpu.make_async_copy(a, b, load_sem.at[i]) for i, (a, b) in enumerate(pairs)]
        for load in loads:
            load.start()
        pairs = [(upg, wg.at[me, 0]), (upv, wg.at[me, 1]), (down, wd.at[me])]
        weight_loads = [
            pltpu.make_async_copy(a, b, load_sem.at[6 + i]) for i, (a, b) in enumerate(pairs)
        ]
        for load in weight_loads:
            pl.when(straight)(load.start)

        barrier = pltpu.get_barrier_semaphore()

        def greet(to_sp, to_tp, cond=None):
            def go():
                pl.semaphore_signal(barrier, inc=1, device_id=(to_sp, to_tp), device_id_type=MESH)

            if cond is None:
                go()
            else:
                pl.when(cond)(go)

        other_y = [z * ny + (y + d) % ny for d in range(1, ny)]
        last_x = jnp.logical_and(c == 1, x == lines - 1)
        next_sp = jnp.where(last_x, sp + 1, sp)
        next_x = jnp.where(c == 0, x, jnp.where(last_x, 0, x + 1))
        has_next = jnp.logical_or(jnp.logical_not(last_x), sp < n_sp - 1)
        next_z = next_sp // ny
        next_seg = next_sp % ny * lines + next_x
        halo_to = [
            (next_z * ny + yy, xx * cores + 1 - c, has_next) for yy in range(ny) for xx in range(lines)
        ]
        halo_from = []
        for yy in range(ny):
            for xx in range(lines):
                here = z * ny + yy
                if xx > 0:
                    halo_from.append((here, jnp.where(c == 1, xx * cores, (xx - 1) * cores + 1), None))
                else:
                    halo_from.append(
                        (
                            jnp.where(c == 1, here, here - 1),
                            jnp.where(c == 1, 0, (lines - 1) * cores + 1),
                            jnp.logical_or(c == 1, here > 0),
                        )
                    )
        other_c = [x * cores + (c + d) % cores for d in range(1, cores)]
        other_x = [(x + d) % lines * cores + c for d in range(1, lines)]
        peers = [(sp + ny, tp, z < nz - 1), (sp - ny, tp, z > 0)]
        peers += [(o, tp, None) for o in other_y]
        peers += [(sp, o, None) for o in other_c + other_x]
        peers += [(cross_sp, cross_tp, crossed)]
        peers += halo_to + halo_from
        for to_sp, to_tp, cond in peers:
            greet(to_sp, to_tp, cond)
        count = jnp.int32(0)
        for _, _, cond in peers:
            count = count + (1 if cond is None else cond.astype(jnp.int32))
        pl.semaphore_wait(barrier, count)

        bulk = Sends()

        def slot(p, src):
            m, h = p // 2, p % 2
            if m < 2:
                return wg.at[src, m, pl.ds(h * dh, dh)]
            return wd.at[src, pl.ds(h * hh, hh)]

        def mine(p):
            m, h = p // 2, p % 2
            if m == 2:
                return down.at[pl.ds(h * hh, hh)]
            return (upg, upv)[m].at[pl.ds(h * dh, dh)]

        def cross(p, also=None):
            cond = crossed if also is None else jnp.logical_and(crossed, also)
            bulk.start(
                remote(mine(p), slot(p, sp), bulk_y.at[p], bulk_r.at[p, sp], cross_sp, cross_tp), cond
            )

        def own_z(p, up, also=None):
            cond, to = (z < nz - 1, sp + ny) if up else (z > 0, sp - ny)
            cond = jnp.logical_and(cond, straight)
            if also is not None:
                cond = jnp.logical_and(cond, also)
            bulk.start(
                remote(mine(p), slot(p, me), bulk_z.at[p, z if up else nz], bulk_r.at[p, me], to, tp),
                cond,
            )

        def own_c(p):
            bulk.start(
                remote(mine(p), slot(p, me), bulk_c.at[p, z], bulk_r.at[p, me], sp, by_c), straight
            )

        def crossed_own(p, also=None):
            go = crossed if also is None else jnp.logical_and(crossed, also)
            arrived(slot(p, me), bulk_y.at[p], bulk_r.at[p, me], go)
            for up in (False, True):
                cond, to = (z < nz - 1, sp + ny) if up else (z > 0, sp - ny)
                bulk.start(
                    remote(
                        slot(p, me), slot(p, me), bulk_z.at[p, z if up else nz], bulk_r.at[p, me], to, tp
                    ),
                    jnp.logical_and(cond, go),
                )
            bulk.start(
                remote(slot(p, me), slot(p, me), bulk_c.at[p, z], bulk_r.at[p, me], sp, by_c), go
            )

        middle = jnp.logical_and(z > 0, z < nz - 1)

        def source(up, d, also=None):
            src, cond = (me - d * ny, z >= d) if up else (me + d * ny, z < nz - d)
            return src, cond if also is None else jnp.logical_and(cond, also)

        def take(p, up, d, also=None):
            src, cond = source(up, d, also)
            src = jnp.clip(src, 0, n_sp - 1)
            arrived(slot(p, src), bulk_z.at[p, 0], bulk_r.at[p, src], cond)

        def on_z(p, up, d, also=None):
            src, cond = source(up, d, also)
            src = jnp.clip(src, 0, n_sp - 1)
            to, more = (sp + ny, z < nz - 1) if up else (sp - ny, z > 0)
            sem = bulk_z.at[p, src // ny]
            bulk.start(
                remote(slot(p, src), slot(p, src), sem, bulk_r.at[p, src], to, tp),
                jnp.logical_and(cond, more),
            )

        def on_c(p, up, d, also=None):
            src, cond = source(up, d, also)
            src = jnp.clip(src, 0, n_sp - 1)
            sem = bulk_c.at[p, src // ny]
            bulk.start(
                remote(slot(p, src), slot(p, src), sem, bulk_r.at[p, src], sp, by_c), cond
            )

        def relay(m, up, d, also=None):
            if d >= nz:
                return
            for p in (2 * m, 2 * m + 1):
                take(p, up, d, also)
                if d < nz - 1:
                    on_z(p, up, d, also)
                on_c(p, up, d, also)

        def side_arrivals(m):
            for zz in range(nz):
                for p in (2 * m, 2 * m + 1):
                    src = zz * ny + 1 - c
                    arrived(slot(p, src), bulk_z.at[p, 0], bulk_r.at[p, src])

        own_z(0, True)
        own_z(1, True, z > 0)
        own_z(2, True, z > 0)
        own_z(3, True, z > 1)
        for p in (0, 1, 2, 3):
            own_z(p, False)
        cross(0)

        ii = lax.broadcasted_iota(jnp.int32, (BLOCK, BLOCK), 0)
        jj = lax.broadcasted_iota(jnp.int32, (BLOCK, BLOCK), 1)
        lower = (ii >= jj).astype(F32)
        logs = log_ref[...]
        cum_col[...] = dot_t(lower, logs, ((1,), (1,)), lax.Precision.HIGHEST)

        def column(idx):
            lane = lax.broadcasted_iota(jnp.int32, cum_col.shape, 1)
            return jnp.sum(jnp.where(lane == idx, cum_col[...], 0.0), axis=1, keepdims=True)

        def angles(b):
            row = pl.ds(sp * nb + b, 1)
            co, so = cos_out[row, :], sin_out[row, :]
            ci, si = cos_in[...], sin_in[...]
            return ci * co - si * so, si * co + ci * so

        def rotated(value, cosine, sine):
            front, second = value[:, :half_k], value[:, half_k:]
            return jnp.concatenate(
                [front * cosine - second * sine, front * sine + second * cosine], axis=1
            )

        def block_rows(b):
            return pl.ds(pl.multiple_of(b * BLOCK, BLOCK), BLOCK)

        loads[0].wait()
        loads[1].wait()
        st[...] = jnp.zeros_like(st)

        def local_states(b, _):
            r = block_rows(b)
            cosine, sine = angles(b)
            for h in range(heads):
                cc = column(h * nb + b)
                total = cc[BLOCK - 1 : BLOCK, :]
                kc = pl.ds(h * key_width, key_width)
                key = rotated(kb[r, kc].astype(F32), cosine, sine) * key_width ** (-0.5)
                key = key.astype(BF16)
                kb[r, kc] = key
                faded = (key.astype(F32) * jnp.exp(total - cc)).astype(BF16)
                term = dot_t(faded, vb[r, pl.ds(h * value_width, value_width)], ((0,), (0,)))
                before = st[h]
                lb[b * heads + h] = before.astype(BF16)
                st[h] = jnp.exp(total) * before + term
            return 0

        lax.fori_loop(0, nb, local_states, 0)

        def head_log(h):
            total = jnp.zeros((1, 1), F32)
            for b in range(nb):
                total = total + jnp.sum(logs[h * nb + b : h * nb + b + 1, :], axis=1, keepdims=True)
            return total

        hrow = lax.broadcasted_iota(jnp.int32, (8, 128), 0)
        tile = jnp.zeros((8, 128), F32)
        for h in range(heads):
            tile = jnp.where(hrow == h, head_log(h), tile)
        dec[pl.ds(y, 1)] = tile[None]
        states = Sends()
        for d, to in enumerate(other_y):
            far = (y + d + 1) % ny
            states.start(
                remote(dec.at[y], dec.at[y], dec_s.at[d], dec_r.at[y], to, tp)
            )
            for h in range(heads):
                for f in range(ny):

                    @pl.when(far == f)
                    def _():
                        xs[d, h] = st[h, :, f * slice_w : (f + 1) * slice_w].astype(BF16)

                states.start(
                    remote(xs.at[d, h], xr.at[y, h], st_s.at[d, h], st_r.at[y, h], to, tp)
                )
        cross(1)
        upper = z >= nz // 2
        cross(2, upper)
        cross(3, upper)

        loads[2].wait()

        def within_block(b, _):
            r = block_rows(b)
            cosine, sine = angles(b)
            for h in range(heads):
                cc = column(h * nb + b)
                kc = pl.ds(h * key_width, key_width)
                query = rotated(qb[r, kc].astype(F32), cosine, sine).astype(BF16)
                scores = dot_t(query, kb[r, kc], ((1,), (1,)))
                crow = jnp.sum(jnp.where(ii == jj, cc, 0.0), axis=0, keepdims=True)
                gap = jnp.where(ii >= jj, cc - crow, 0.0)
                weight = jnp.where(ii >= jj, jnp.exp(gap), 0.0)
                vc = pl.ds(h * value_width, value_width)
                within[r, vc] = dot((scores * weight).astype(BF16), vb[r, vc])
                qb[r, kc] = (query.astype(F32) * jnp.exp(cc)).astype(BF16)
            return 0

        lax.fori_loop(0, nb, within_block, 0)
        crossed_own(0)

        for f in range(ny):

            @pl.when(y == f)
            def _():
                for h in range(heads):
                    xr[f, h] = st[h, :, f * slice_w : (f + 1) * slice_w].astype(BF16)

        for d in range(1, ny):
            src = (y + d) % ny
            arrived(dec.at[src], dec_s.at[0], dec_r.at[src])
            for h in range(heads):
                arrived(xr.at[src, h], st_s.at[0, 0], st_r.at[src, h])
        crossed_own(1, upper)
        for h in range(heads):

            @pl.when(z == 0)
            def _():
                chain_r[h] = jnp.zeros((key_width, slice_w), BF16)

            arrived(chain_r.at[h], ch_s.at[h], ch_r.at[h], z > 0)
            incoming = chain_r[h].astype(F32)
            before = incoming
            for f in range(ny):
                cb_mine = before.astype(BF16)

                @pl.when(y == f)
                def _():
                    cb[y, h] = cb_mine

                @pl.when(y != f)
                def _():
                    cs[f, h] = cb_mine

                decay = jnp.exp(dec[f, h : h + 1, 0:1])
                before = decay * before + xr[f, h].astype(F32)
            chain_s[h] = before.astype(BF16)
            states.start(
                remote(chain_s.at[h], chain_r.at[h], ch_s.at[h], ch_r.at[h], sp + ny, tp),
                z < nz - 1,
            )
            for d, to in enumerate(other_y):
                far = (y + d + 1) % ny
                states.start(
                    remote(cs.at[far, h], cb.at[y, h], cb_s.at[d, h], cb_r.at[y, h], to, tp)
                )

        own_z(1, True, z == 0)
        own_z(2, True, z == 0)
        own_z(3, True, z <= 1)
        for p in range(4):
            own_c(p)
        for p in (2, 3):
            cross(p, jnp.logical_not(upper))
        for p in (4, 5):
            cross(p)
        bulk.start(remote(taps, tapb, tap_s.at[0], tap_r.at[0], cross_sp, cross_tp), crossed)
        bulk.start(remote(shift, shiftb, tap_s.at[1], tap_r.at[1], cross_sp, cross_tp), crossed)

        @pl.when(straight)
        def _():
            tapb[...] = taps[...]
            shiftb[...] = shift[...]

        crossed_own(1, jnp.logical_not(upper))
        crossed_own(2, upper)
        crossed_own(3, upper)
        relay(0, False, 1, straight)
        for p in (4, 5):
            own_z(p, False)
            own_z(p, True)
            own_c(p)

        loads[3].wait()
        for h in range(heads):
            for d in range(1, ny):
                src = (y + d) % ny
                arrived(cb.at[src, h], cb_s.at[0, 0], cb_r.at[src, h])

            def finish(b, decay):
                r = block_rows(b)
                vc = pl.ds(h * value_width, value_width)
                state = jnp.concatenate([cb[f, h].astype(F32) for f in range(ny)], axis=1)
                state = (decay * state + lb[b * heads + h].astype(F32)).astype(BF16)
                mixed = within[r, vc] + dot(qb[r, pl.ds(h * key_width, key_width)], state)
                average = jnp.mean(mixed, axis=1, keepdims=True)
                mixed = mixed - average
                spread = jnp.mean(mixed * mixed, axis=1, keepdims=True)
                gate = gb[r, vc].astype(F32)
                gated = gate * jax.nn.sigmoid(gate) * (mixed * lax.rsqrt(spread + tiny_stabilizer))
                gb[r, vc] = gated.astype(BF16)
                return decay * jnp.exp(column(h * nb + b)[BLOCK - 1 : BLOCK, :])

            lax.fori_loop(0, nb, finish, jnp.ones((1, 1), F32))
        states.drain()

        def owner_rows(xx, cc):
            return pl.ds(pl.multiple_of((xx * cores + cc) * own, own), own)

        def piece_cols(s):
            return pl.ds(pl.multiple_of(s * piece, piece), piece)

        def d2d_copies(s):
            return [
                remote(
                    part.at[s, owner_rows(xx, (c + d) % cores)], r1.at[s, d - 1, xx],
                    f1_s.at[s, (d - 1) * lines + xx], f1_r.at[s, (d - 1) * lines + xx],
                    sp, x * cores + (c + d) % cores,
                )
                for d in range(1, cores)
                for xx in range(lines)
            ]

        def x_copies(s):
            return [
                remote(
                    s2.at[s, d - 1], r2.at[s, d - 1], f2_s.at[s, d - 1], f2_r.at[s, d - 1],
                    sp, (x + d) % lines * cores + c,
                )
                for d in range(1, lines)
            ]

        row_tile = min(tok_rows, 512)

        def product(s, lhs, rhs):
            def one(i, _):
                r = pl.ds(pl.multiple_of(i * row_tile, row_tile), row_tile)
                part[s, r, :] = dot(lhs[r, :], rhs()).astype(BF16)
                return 0

            lax.fori_loop(0, tok_rows // row_tile, one, 0)
            for copy in d2d_copies(s):
                copy.start()

        def combine(s):
            for copy in d2d_copies(s):
                copy.wait_recv()
            for d in range(lines):
                xx = (x + d) % lines
                total = part[s, owner_rows(xx, c), :].astype(F32)
                for e in range(cores - 1):
                    total = total + r1[s, e, xx].astype(F32)
                if d == 0:
                    acc[:, piece_cols(s)] = total
                else:
                    s2[s, d - 1] = total.astype(BF16)
            for copy in x_copies(s):
                copy.start()

        def collect(s):
            for copy in x_copies(s):
                copy.wait_recv()
            total = acc[:, piece_cols(s)]
            for d in range(lines - 1):
                total = total + r2[s, d].astype(F32)
            acc[:, piece_cols(s)] = total

        def release(s, _):
            for copy in d2d_copies(s) + x_copies(s):
                copy.wait_send()
            return 0

        def out_step(s, _):
            product(s, gb, lambda: ow[:, piece_cols(s)])
            pl.when(s > 0)(lambda: combine(s - 1))
            return 0

        loads[4].wait()
        lax.fori_loop(0, n_sp, out_step, 0)
        combine(n_sp - 1)
        crossed_own(2, jnp.logical_not(upper))
        crossed_own(3, jnp.logical_not(upper))
        relay(0, False, 1, crossed)
        relay(0, True, 1)
        relay(0, False, 2, straight)
        relay(0, True, 2, straight)
        relay(1, False, 1, straight)
        relay(1, True, 1, straight)

        def collect_step(s, _):
            collect(s)
            return 0

        lax.fori_loop(0, n_sp, collect_step, 0)

        loads[5].wait()

        def layer_norm(values, which):
            average = jnp.mean(values, axis=1, keepdims=True)
            values = values - average
            spread = jnp.mean(values * values, axis=1, keepdims=True)
            values = values * lax.rsqrt(spread + tiny_stabilizer)
            return values * gain[which : which + 1, :] + bias[which : which + 1, :]

        ln_rows = 32
        gathered = Sends()

        seg = HALO + own

        def chunk_of(yy, xx, j):
            at = (yy * lines + xx) * seg + HALO + j * chunk
            return rows.at[pl.ds(pl.multiple_of(at, 16), chunk)]

        def gather_sem(j, yy, xx):
            return ag_r.at[j, yy * lines + xx]

        for yy in range(ny):
            for xx in range(lines):
                if yy == 0 and xx == 0:

                    @pl.when(jnp.logical_and(z == 0, c == 0))
                    def _():
                        rows[pl.ds(0, HALO), :] = jnp.zeros((HALO, width), BF16)

        for j in range(ROW_CHUNKS):

            def norm_rows(i, _):
                at = pl.multiple_of(j * chunk + i * ln_rows, ln_rows)
                r = pl.ds(at, ln_rows)
                value = layer_norm(alpha_scale * res[r, :].astype(F32) + acc[r, :], 0).astype(BF16)
                res[r, :] = value
                rows[pl.ds(pl.multiple_of((y * lines + x) * seg + HALO + at, 16), ln_rows), :] = value
                return 0

            lax.fori_loop(0, chunk // ln_rows, norm_rows, 0)
            mine_now = chunk_of(y, x, j)
            gathered.start(remote(mine_now, mine_now, ag_s.at[j, 0], gather_sem(j, y, x), sp, by_x))
            gathered.start(remote(mine_now, mine_now, ag_s.at[j, 1], gather_sem(j, y, x), by_y, tp))
        tail = rows.at[pl.ds(pl.multiple_of((y * lines + x) * seg + own, 16), HALO)]
        head = rows.at[pl.ds(pl.multiple_of(next_seg * seg, 16), HALO)]
        for t, (to_sp, to_tp, cond) in enumerate(halo_to):
            gathered.start(remote(tail, head, halo_s.at[t], halo_r.at[next_seg], to_sp, to_tp), cond)
        for j in range(ROW_CHUNKS):
            if j == 1:
                relay(0, False, 2, crossed)
                relay(0, True, 2, crossed)
                relay(1, False, 1, crossed)
                relay(1, True, 1, crossed)
            if j == ROW_CHUNKS // 2:
                relay(0, False, 3)
                relay(1, False, 2, z > 0)
                relay(1, True, 2, z < nz - 1)
                crossed_own(4)
                crossed_own(5)
            if j == ROW_CHUNKS - 1:
                relay(0, True, 3)
            got = chunk_of(y, 1 - x, j)
            arrived(got, ag_s.at[j, 0], gather_sem(j, y, 1 - x))
            if j % 2 == 0:
                gathered.start(remote(got, got, ag_s.at[j, 2], gather_sem(j, y, 1 - x), by_y, tp))
            got = chunk_of(1 - y, x, j)
            arrived(got, ag_s.at[j, 0], gather_sem(j, 1 - y, x))
            if j % 2 == 1:
                gathered.start(remote(got, got, ag_s.at[j, 2], gather_sem(j, 1 - y, x), sp, by_x))
        for d in range(4, nz):
            relay(0, False, d)
            relay(0, True, d)
        pl.when(straight)(weight_loads[0].wait)
        side_arrivals(0)
        for g, (_, _, cond) in enumerate(halo_from):
            arrived(rows.at[pl.ds(g * seg, HALO)], halo_s.at[0], halo_r.at[g], cond)

        def up_tile(m, start, count):
            r = pl.ds(start, count)
            total = None
            for s in range(n_sp):
                term = dot(rows[r, s * depth : (s + 1) * depth], wg[s, m])
                total = term if total is None else total + term
            ups[m, r, :] = total.astype(BF16)

        def gate_step(i, _):
            yy = jnp.where(i >= 2, 1 - y, y)
            xx = jnp.where(i % 2 == 1, 1 - x, x)
            up_tile(0, pl.multiple_of((yy * lines + xx) * seg, 16), seg)
            return 0

        lax.fori_loop(0, n_tp - 1, gate_step, 0)
        relay(2, False, 1, jnp.logical_and(middle, straight))
        for j in range(ROW_CHUNKS):
            arrived(chunk_of(1 - y, 1 - x, j), ag_s.at[j, 0], gather_sem(j, 1 - y, 1 - x))
        relay(1, False, 2, z == 0)
        relay(1, True, 2, z == nz - 1)
        lax.fori_loop(0, n_sp, release, 0)

        lax.fori_loop(n_tp - 1, n_tp, gate_step, 0)
        for d in range(3, nz):
            relay(1, False, d)
            relay(1, True, d)
        relay(2, False, 1, jnp.logical_and(middle, crossed))
        relay(2, True, 1, middle)
        pl.when(straight)(weight_loads[1].wait)
        side_arrivals(1)

        arrived(tapb, tap_s.at[0], tap_r.at[0], crossed)
        arrived(shiftb, tap_s.at[1], tap_r.at[1], crossed)

        def activate(i, col):
            at = pl.multiple_of(i * seg, 16)
            convs = []
            for m in range(2):
                tile = ups[m, pl.ds(at, seg), col].astype(F32)
                value = shiftb[m : m + 1, col]
                for j in range(3):
                    value = value + tapb[m, j : j + 1, col] * tile[HALO - 2 + j : HALO - 2 + j + own, :]
                convs.append(value)
            act[pl.ds(pl.multiple_of(i * own, 16), own), col] = (
                jax.nn.gelu(convs[0]) * convs[1]
            ).astype(BF16)

        order = [
            [zz] + sorted((o for o in range(nz) if o != zz), key=lambda o: (abs(o - zz), abs(2 * o - nz + 1)))
            for zz in range(nz)
        ]

        def nearest(k):
            got = jnp.int32(order[0][k])
            for zz in range(1, nz):
                got = jnp.where(z == zz, order[zz][k], got)
            return got

        half = piece // 2
        left, right = pl.ds(0, half), pl.ds(half, half)

        def seg_rows(yy, xx):
            return pl.ds(pl.multiple_of((yy * lines + xx) * own, own), own)

        def over_x(s, yy):
            return remote(
                part.at[s, seg_rows(yy, 1 - x), left], r1.at[s, 0, yy, :, left],
                f1_s.at[s, yy], f1_r.at[s, yy], sp, by_x,
            )

        def over_y(s, xx):
            return remote(
                part.at[s, seg_rows(1 - y, xx), right], r1.at[s, 0, xx, :, right],
                f1_s.at[s, ny + xx], f1_r.at[s, ny + xx], by_y, tp,
            )

        def first_hops(s):
            return [over_x(s, yy) for yy in range(ny)] + [over_y(s, xx) for xx in range(lines)]

        def second_hops(s):
            return [
                remote(
                    s2.at[s, 0, :, left], r2.at[s, 0, :, left], f2_s.at[s, 0], f2_r.at[s, 0], by_y, tp
                ),
                remote(
                    s2.at[s, 0, :, right], r2.at[s, 0, :, right], f2_s.at[s, 1], f2_r.at[s, 1], sp, by_x
                ),
            ]

        def halves(s):
            at = pl.multiple_of(s * piece, piece)
            return pl.ds(at, half), pl.ds(pl.multiple_of(at + half, half), half)

        def down_step(s):
            def one(i, _):
                r = pl.ds(pl.multiple_of(i * row_tile, row_tile), row_tile)
                part[s, r, :] = dot(act[r, :], wd[s]).astype(BF16)
                return 0

            lax.fori_loop(0, tok_rows // row_tile, one, 0)
            for copy in first_hops(s):
                copy.start()

        def down_combine(s):
            for copy in first_hops(s):
                copy.wait_recv()
            lcols, rcols = halves(s)

            def summed(yy, xx, other, cols):
                return part[s, seg_rows(yy, xx), cols].astype(F32) + r1[s, 0, other, :, cols].astype(F32)

            s2[s, 0, :, left] = summed(1 - y, x, 1 - y, left).astype(BF16)
            s2[s, 0, :, right] = summed(y, 1 - x, 1 - x, right).astype(BF16)
            for copy in second_hops(s):
                copy.start()
            acc[:, lcols] = summed(y, x, y, left)
            acc[:, rcols] = summed(y, x, x, right)

        def down_collect(s):
            for copy in second_hops(s):
                copy.wait_recv()
            acc[:, piece_cols(s)] = acc[:, piece_cols(s)] + r2[s, 0].astype(F32)

        def down_release(s, _):
            for copy in first_hops(s) + second_hops(s):
                copy.wait_send()
            return 0

        pl.when(straight)(weight_loads[2].wait)
        for p in (4, 5):
            arrived(slot(p, z * ny + 1 - c), bulk_z.at[p, 0], bulk_r.at[p, z * ny + 1 - c])
        early = [me, z * ny + 1 - c]

        def value_step(i, _):
            to_y, to_x = i % 2 == 0, i < 2
            yy = jnp.where(to_y, 1 - y, y)
            xx = jnp.where(to_x, 1 - x, x)
            g = yy * lines + xx
            up_tile(1, pl.multiple_of(g * seg, 16), seg)
            for t in range(hidden // hcols):
                activate(g, pl.ds(t * hcols, hcols))
            r = seg_rows(yy, xx)
            for s in early:
                part[s, r, :] = dot(act[r, :], wd[s]).astype(BF16)
                pl.when(to_x)(over_x(s, yy).start)
                pl.when(to_y)(over_y(s, xx).start)
            return 0

        lax.fori_loop(0, n_tp, value_step, 0)
        for d in range(2, nz - 1):
            relay(2, False, d, middle)
            relay(2, True, d, middle)
        for s in early:
            down_combine(s)
        previous = None
        done = list(early)
        for k in range(1, nz):
            src_z = nearest(k)
            src = src_z * ny + c
            fresh = jnp.logical_not(middle)
            for p in (4, 5):
                arrived(slot(p, src), bulk_z.at[p, 0], bulk_r.at[p, src], fresh)
                bulk.start(
                    remote(
                        slot(p, src), slot(p, src), bulk_c.at[p, src_z],
                        bulk_r.at[p, src], sp, by_c,
                    ),
                    fresh,
                )
            for d in range(cores):
                src = src_z * ny + (c + d) % cores
                if d > 0:
                    for p in (4, 5):
                        arrived(slot(p, src), bulk_z.at[p, 0], bulk_r.at[p, src])
                down_step(src)
                if previous is not None:
                    down_combine(previous)
                previous = src
                done.append(src)
        down_combine(previous)
        for src in done:
            down_collect(src)

        def final_rows(i, _):
            r = pl.ds(pl.multiple_of(i * ln_rows, ln_rows), ln_rows)
            out[r, :] = layer_norm(alpha_scale * res[r, :].astype(F32) + acc[r, :], 1).astype(BF16)
            return 0

        lax.fori_loop(0, own // ln_rows, final_rows, 0)
        lax.fori_loop(0, n_sp, down_release, 0)
        gathered.drain()
        bulk.drain()

    vmem, dma = pltpu.VMEM, pltpu.SemaphoreType.DMA
    oc, ol, oy = max(cores - 1, 1), max(lines - 1, 1), max(ny - 1, 1)
    scratch = [
        vmem((2, 3, hidden), F32),
        vmem((2, hidden), F32),
        vmem((n_sp, 2, depth, hidden), BF16),
        vmem((n_sp, hidden, piece), BF16),
        vmem((tok_rows, heads * key_width), BF16),
        vmem((tok_rows, heads * key_width), BF16),
        vmem((tok_rows, heads * value_width), BF16),
        vmem((tok_rows, heads * value_width), BF16),
        vmem((heads * value_width, width), BF16),
        vmem((own, width), BF16),
        vmem((BLOCK, heads * nb), F32),
        vmem((heads, key_width, value_width), F32),
        vmem((nb * heads, key_width, value_width), BF16),
        vmem((tok_rows, heads * value_width), F32),
        vmem((oy, heads, key_width, slice_w), BF16),
        vmem((ny, heads, key_width, slice_w), BF16),
        vmem((ny, 8, 128), F32),
        vmem((heads, key_width, slice_w), BF16),
        vmem((heads, key_width, slice_w), BF16),
        vmem((ny, heads, key_width, slice_w), BF16),
        vmem((ny, heads, key_width, slice_w), BF16),
        vmem((n_sp, tok_rows, piece), BF16),
        vmem((n_sp, oc, lines, own, piece), BF16),
        vmem((n_sp, ol, own, piece), BF16),
        vmem((n_sp, ol, own, piece), BF16),
        vmem((own, width), F32),
        vmem((n_tp * HALO + tok_rows, width), BF16),
        vmem((2, n_tp * HALO + tok_rows, hidden), BF16),
        vmem((tok_rows, hidden), BF16),
        dma((9,)),
        dma((6, n_sp)),
        dma((6, nz + 1)),
        dma((6,)),
        dma((6, nz)),
        dma((2,)),
        dma((2,)),
        dma((oy, heads)),
        dma((ny, heads)),
        dma((oy,)),
        dma((ny,)),
        dma((heads,)),
        dma((heads,)),
        dma((oy, heads)),
        dma((ny, heads)),
        dma((ROW_CHUNKS, 3)),
        dma((ROW_CHUNKS, n_tp)),
        dma((n_tp,)),
        dma((n_tp,)),
        dma((n_sp, ny + lines)),
        dma((n_sp, ny + lines)),
        dma((n_sp, 2)),
        dma((n_sp, 2)),
    ]
    in_specs = [pl.BlockSpec(memory_space=pltpu.VMEM)] * 9 + [pl.BlockSpec(memory_space=pl.ANY)] * 9
    return pl.pallas_call(
        kernel,
        out_shape=jax.ShapeDtypeStruct((own, width), BF16),
        in_specs=in_specs,
        out_specs=pl.BlockSpec(memory_space=pltpu.VMEM),
        scratch_shapes=scratch,
        compiler_params=pltpu.CompilerParams(
            collective_id=0, has_side_effects=True, vmem_limit_bytes=67_000_000
        ),
    )


def shards(
    query_proj, key_proj, value_proj, gate_proj, log_decay, residual, out_weight, norm_gain,
    norm_bias, up_gate, up_value, conv_weight, conv_bias, down_weight,
):
    n_sp, n_tp = lax.axis_size("sp"), lax.axis_size("tp")
    tok_rows, heads = log_decay.shape
    key_width = query_proj.shape[1] // heads
    value_width = value_proj.shape[1] // heads
    nb = tok_rows // BLOCK
    cores, lines, ny, _ = layout(n_sp, n_tp)
    make = make_square_kernel if cores == lines == ny == 2 else make_kernel
    call = make(
        n_sp, n_tp, tok_rows, heads, key_width, value_width,
        residual.shape[1], up_gate.shape[0], up_gate.shape[1],
    )
    tables = rotary_tables(key_width, n_sp * nb)
    logs = log_decay.T.reshape(heads * nb, BLOCK)
    return call(
        *tables, logs, norm_gain, norm_bias, conv_weight, conv_bias, query_proj, key_proj,
        value_proj, gate_proj, residual, out_weight, up_gate, up_value, down_weight,
    )


def solution(mesh):
    placed = (
        P("sp", "tp"), P("sp", "tp"), P("sp", "tp"), P("sp", "tp"), P("sp", "tp"),
        P("sp", None), P("tp", None), P(), P(), P("sp", "tp"), P("sp", "tp"),
        P(None, None, "tp"), P(None, "tp"), P("tp", "sp"),
    )
    return jax.shard_map(
        shards, mesh=mesh, in_specs=placed, out_specs=P(("sp", "tp"), None), check_vma=False
    )
```
